128 devices in a mesh: sp: 16 (over z, x), dp: 8 (over y, core).
Axes of the slice: x: 4, y: 4, z: 4, core: 2. Of those that a mesh axis runs over, the one named last changes fastest.
Arguments:
- residual: bfloat16 [8, 2048, 2048], P('dp', 'sp'), may hold values from -6 to 6
- query_projected: bfloat16 [8, 2048, 1024], P('dp', 'sp'), may hold values from -6 to 6
- key_projected: bfloat16 [8, 2048, 1024], P('dp', 'sp'), may hold values from -6 to 6
- value_projected: bfloat16 [8, 2048, 1024], P('dp', 'sp'), may hold values from -6 to 6
- output_gate_proj: bfloat16 [8, 2048, 1024], P('dp', 'sp'), may hold values from -6 to 6
- write_strength_logits: float32 [8, 2048, 16], P('dp', 'sp'), may hold values from -6 to 6
- decay_logits: float32 [8, 2048, 16], P('dp', 'sp'), may hold values from -5 to 5
- extra_log_decay: float32 [8, 2048, 16], P('dp', 'sp'), may hold values from -0.7 to 0
- head_decay_rate: float32 [16], P('sp'), may hold values from 0 to 0.06
- head_norm_gain: float32 [64], replicated, may hold values from 0.1 to 1.9
- output_matrix: bfloat16 [1024, 2048], replicated, may hold values from -0.1875 to 0.1875
- expert_norm_gain: float32 [2048], replicated, may hold values from 0.1 to 1.9
- group_router_scores: float32 [8, 2048, 4], P('dp', 'sp'), may hold values from -6 to 6
- chosen_expert_scores: float32 [8, 2048, 2], P('dp', 'sp'), may hold values from -6 to 6
- routes: int32 [8, 2048, 2], P('dp', 'sp'), may hold values from 0 to 127, as said below
- gate_weight: bfloat16 [128, 2048, 1024], P(('sp', 'dp')), may hold values from -0.125 to 0.125
- up_weight: bfloat16 [128, 2048, 1024], P(('sp', 'dp')), may hold values from -0.125 to 0.125
- down_weight: bfloat16 [128, 1024, 2048], P(('sp', 'dp')), may hold values from -0.75 to 0.75
Outputs:
- layer_out: bfloat16 [8, 2048, 2048], P('dp', 'sp')
The draws below stay inside these ranges and needn't reach their ends.
Inputs may be any that keep to these rules, and one draw needn't show every extreme that they name: `routes`: the 2 numbers of a row differ and lie in one group of 32 consecutive experts. Among the rows of one device no expert is named more than 4 times, some expert exactly 4 times, and each group is named by exactly 32 rows.
All inputs are finite; a program needn't handle non-finite values.
Results may differ from the reference program's by a relative error of at most 0.0059.
Values may be sent and summed in bfloat16 or wider, within the bound.
A program may use at most 128 MiB of HBM per device.

```python
import math
import jax
import jax.numpy as jnp
from jax import lax

D = 2048
HEADS = 16
HD = 64
FF_E = 1024
GROUPS = 4
TOPK = 2
BLK = 64
TOK_DEV = 128
SEQS = 8
LEN = 2048
EXPERTS = 128


def route_block(key):
    half = 2 * TOK_DEV // EXPERTS
    per_group = EXPERTS // GROUPS
    first, second, third, fourth = jax.random.split(key, 4)
    perms = jax.vmap(lambda sub: jax.random.permutation(sub, per_group))(jax.random.split(first, GROUPS))
    expert_ids = (perms + jnp.arange(GROUPS, dtype=jnp.int32)[:, None] * per_group).astype(jnp.int32)
    deltas = jax.random.randint(second, (GROUPS, per_group // 2), 0, half + 1)
    deltas = deltas.at[0, 0].set(half)
    counts = jnp.zeros((EXPERTS,), jnp.int32)
    counts = counts.at[expert_ids[:, 0::2]].add(half + deltas)
    counts = counts.at[expert_ids[:, 1::2]].add(half - deltas)
    listed = jnp.repeat(jnp.arange(EXPERTS, dtype=jnp.int32), counts, total_repeat_length=2 * TOK_DEV)
    group_len = per_group * half
    pairs = listed.reshape(GROUPS, 2, group_len // 2).transpose(0, 2, 1).reshape(TOK_DEV, 2)
    flip = jax.random.randint(third, (TOK_DEV,), 0, 2)
    pairs = jnp.where(flip[:, None] == 1, pairs[:, ::-1], pairs)
    order = jax.random.permutation(fourth, TOK_DEV)
    return pairs[order]


def draw_routes(key, part):
    nblocks = SEQS * (LEN // TOK_DEV)
    blocks = jax.vmap(route_block)(jax.random.split(jax.random.fold_in(key, 11), nblocks))
    return blocks.reshape(SEQS, LEN, 2).astype(jnp.int32)


def draw_head_decay_rate(key, part):
    first, second = jax.random.split(jax.random.fold_in(key, 23))
    index = jax.random.permutation(first, HEADS)
    spread = jax.random.uniform(second, (HEADS,), jnp.float32)
    fast = jnp.exp(math.log(0.02) + spread * (math.log(0.06) - math.log(0.02)))
    slow = (0.1 + 0.3 * spread) / LEN
    nfast = HEADS // 2
    return jnp.where(index < nfast, fast, slow).astype(jnp.float32)


def draw_decay_logits(key, part):
    first, second = jax.random.split(jax.random.fold_in(key, 37))
    nblocks = LEN // TOK_DEV
    offset = jax.random.uniform(first, (SEQS, nblocks, 1, 1), jnp.float32, -1.0, 1.0)
    noise = jnp.clip(jax.random.normal(second, (SEQS, nblocks, TOK_DEV, HEADS), jnp.float32), -4.0, 4.0)
    return (noise + offset).reshape(SEQS, LEN, HEADS)


def draw_extra_log_decay(key, part):
    first, second = jax.random.split(jax.random.fold_in(key, 41))
    places = jax.random.randint(first, (SEQS, 2), 0, LEN)
    hit = jnp.any(jnp.arange(LEN, dtype=jnp.int32)[None, :, None] == places[:, None, :], axis=-1)
    strength = jax.random.uniform(second, (SEQS, LEN, HEADS), jnp.float32, math.log(0.5), math.log(0.8))
    return jnp.where(hit[..., None], strength, 0.0).astype(jnp.float32)


def shard_levels(own_key, extent, shards, low, largest):
    factor_of, own = 1.0, jax.random.fold_in(own_key, 6)
    for axis_at, blocks in shards:
        draws = jnp.exp(jax.random.uniform(jax.random.fold_in(own, axis_at), (blocks,), jnp.float32, low / len(shards), largest / len(shards)))
        factor_of = factor_of * jnp.repeat(draws, extent[axis_at] // blocks).reshape([-1 if axis == axis_at else 1 for axis in range(len(extent))])
    return factor_of


def normal_values(rng, extent, scale, limit, cuts=(), kind=jnp.bfloat16):
    values = scale * jax.random.normal(rng, extent, jnp.float32)
    if cuts:
        values = values * shard_levels(rng, extent, cuts, -0.22, 0.18)
    return jnp.clip(values, -limit, limit).astype(kind)


def setup_inputs(seed: int = 0) -> dict:
    streams_of = jax.random.split(jax.random.key(seed), 19)
    return {
        "residual": normal_values(streams_of[0], (SEQS, LEN, D), 1.0, 6.0, ((0, 8), (1, 16))),
        "query_projected": normal_values(streams_of[1], (SEQS, LEN, HEADS * HD), 1.0, 6.0, ((0, 8), (1, 16))),
        "key_projected": normal_values(streams_of[2], (SEQS, LEN, HEADS * HD), 1.0, 6.0, ((0, 8), (1, 16))),
        "value_projected": normal_values(streams_of[3], (SEQS, LEN, HEADS * HD), 1.0, 6.0, ((0, 8), (1, 16))),
        "output_gate_proj": normal_values(streams_of[4], (SEQS, LEN, HEADS * HD), 1.0, 6.0, ((0, 8), (1, 16))),
        "write_strength_logits": normal_values(streams_of[5], (SEQS, LEN, HEADS), 1.0, 6.0, ((0, 8), (1, 16)), jnp.float32),
        "decay_logits": draw_decay_logits(jax.random.fold_in(streams_of[18], 71), 0),
        "extra_log_decay": draw_extra_log_decay(jax.random.fold_in(streams_of[18], 71), 0),
        "head_decay_rate": draw_head_decay_rate(jax.random.fold_in(streams_of[18], 71), 0),
        "head_norm_gain": jnp.clip(1.0 + 0.18 * jax.random.normal(streams_of[9], (HD,), jnp.float32), 0.1, 1.9),
        "output_matrix": normal_values(streams_of[10], (HEADS * HD, D), (HEADS * HD) ** -0.5, 0.1875),
        "expert_norm_gain": jnp.clip(1.0 + 0.18 * jax.random.normal(streams_of[11], (D,), jnp.float32), 0.1, 1.9),
        "group_router_scores": normal_values(streams_of[12], (SEQS, LEN, GROUPS), 1.5, 6.0, ((0, 8), (1, 16)), jnp.float32),
        "chosen_expert_scores": normal_values(streams_of[13], (SEQS, LEN, TOPK), 1.0, 6.0, ((0, 8), (1, 16)), jnp.float32),
        "routes": draw_routes(jax.random.fold_in(streams_of[18], 71), 0),
        "gate_weight": normal_values(streams_of[15], (EXPERTS, D, FF_E), D ** -0.5, 0.125, ((0, 128),)),
        "up_weight": normal_values(streams_of[16], (EXPERTS, D, FF_E), D ** -0.5, 0.125, ((0, 128),)),
        "down_weight": normal_values(streams_of[17], (EXPERTS, FF_E, D), (FF_E // 16) ** -0.5, 0.75, ((0, 128),)),
    }


eps = 1e-06
block_rows = 256

def unit_rows(array):
    return array * lax.rsqrt(lax.optimization_barrier(jnp.sum(array * array, axis=-1, keepdims=True)) + eps)

def block_terms(query, keyed, valued, beta, log_decay_total, span):
    length, width = query.shape
    count = length // span
    highest_precision = lax.Precision.HIGHEST
    qb = query.reshape(count, span, width)
    kb = keyed.reshape(count, span, width)
    vb = valued.reshape(count, span, width)
    bb = beta.reshape(count, span)
    cumul = jnp.cumsum(log_decay_total.reshape(count, span), axis=1)
    rows = jnp.arange(span, dtype=jnp.int32)
    causal = rows[:, None] >= rows[None, :]
    strict = rows[:, None] > rows[None, :]
    diff = cumul[:, :, None] - cumul[:, None, :]
    decay = jnp.where(causal, jnp.exp(jnp.where(causal, diff, 0.0)), 0.0)
    kbeta = kb * bb[..., None]
    lower = jnp.where(strict, jnp.einsum('nid,njd->nij', kbeta, kb, precision=highest_precision) * decay, 0.0)
    rhs = jnp.concatenate([vb * bb[..., None], kbeta * jnp.exp(cumul)[..., None]], axis=-1)
    solved = jax.scipy.linalg.solve_triangular(lower, rhs, lower=True, unit_diagonal=True)
    state_update = solved[..., :width]
    write_decayed = solved[..., width:]
    attention_out = jnp.einsum('nid,njd->nij', qb, kb, precision=highest_precision) * decay
    query_decayed = qb * jnp.exp(cumul)[..., None]
    key_decayed = kb * jnp.exp(cumul[:, -1:] - cumul)[..., None]
    total = jnp.exp(cumul[:, -1])
    return (attention_out, query_decayed, write_decayed, state_update, key_decayed, total)

def run_head(args):
    query, keyed, valued, beta, log_decay_total = args
    length, width = query.shape
    highest_precision = lax.Precision.HIGHEST
    terms = block_terms(query, keyed, valued, beta, log_decay_total, BLK)

    def advance(state, inputs):
        attention_out, query_decayed, write_decayed, state_update, key_decayed, total = inputs
        value_corrected = state_update - jnp.dot(write_decayed, state, precision=highest_precision)
        final_output = jnp.dot(query_decayed, state, precision=highest_precision) + jnp.dot(attention_out, value_corrected, precision=highest_precision)
        state = state * total + jnp.dot(key_decayed.T, value_corrected, precision=highest_precision)
        return (state, final_output)
    _, outputs = lax.scan(advance, jnp.zeros((width, width), jnp.float32), terms)
    return outputs.reshape(length, width)

def routed(ffn_in, chosen, gate_weight, up_weight, down_weight):
    ntok, width = ffn_in.shape
    experts = gate_weight.shape[0]
    nassign = ntok * 2
    eid = chosen.reshape(nassign).astype(jnp.int32)
    order = jnp.argsort(eid, stable=True).astype(jnp.int32)
    eid_sorted = eid[order]
    counts = jnp.zeros((experts,), jnp.int32).at[eid].add(1)
    padded = (counts + block_rows - 1) // block_rows * block_rows
    start = (jnp.cumsum(counts) - counts).astype(jnp.int32)
    pend = jnp.cumsum(padded).astype(jnp.int32)
    pstart = pend - padded
    dest = pstart[eid_sorted] + jnp.arange(nassign, dtype=jnp.int32) - start[eid_sorted]
    total = nassign + experts * block_rows
    nblocks = total // block_rows
    slot_assign = jnp.full((total,), nassign, jnp.int32).at[dest].set(order)
    slot_tok = jnp.where(slot_assign < nassign, slot_assign // 2, ntok).astype(jnp.int32)
    rows = jnp.take(ffn_in, slot_tok, axis=0, mode='fill', fill_value=0).reshape(nblocks, block_rows, width)
    block_expert = jnp.minimum(jnp.searchsorted(pend, jnp.arange(nblocks, dtype=jnp.int32) * block_rows, side='right'), experts - 1).astype(jnp.int32)

    def one_block(args):
        xblock, expert = args
        gate = jnp.dot(xblock.astype(jnp.float32), gate_weight[expert].astype(jnp.float32), preferred_element_type=jnp.float32)
        upper = jnp.dot(xblock.astype(jnp.float32), up_weight[expert].astype(jnp.float32), preferred_element_type=jnp.float32)
        hidden = (jax.nn.silu(gate) * upper).astype(jnp.bfloat16)
        return jnp.dot(hidden.astype(jnp.float32), down_weight[expert].astype(jnp.float32), preferred_element_type=jnp.float32).astype(jnp.bfloat16)
    outputs = lax.map(one_block, (rows, block_expert)).reshape(total, width)
    per_assign = jnp.zeros((nassign + 1, width), jnp.bfloat16).at[slot_assign].set(outputs)[:nassign]
    return per_assign.reshape(ntok, 2, width)

def reference(residual, query_projected, key_projected, value_projected, output_gate_proj, write_strength_logits, decay_logits, extra_log_decay, head_decay_rate, head_norm_gain, output_matrix, expert_norm_gain, group_router_scores, chosen_expert_scores, routes, gate_weight, up_weight, down_weight):
    seqs, length, joined = query_projected.shape
    heads = head_decay_rate.shape[0]
    width = joined // heads
    model = residual.shape[-1]

    def heads_of(array):
        return array.astype(jnp.float32).reshape(seqs, length, heads, width).transpose(0, 2, 1, 3).reshape(seqs * heads, length, width)
    query = unit_rows(heads_of(query_projected)) * width ** (-0.5)
    keyed = unit_rows(heads_of(key_projected))
    valued = heads_of(value_projected)
    beta = jax.nn.sigmoid(write_strength_logits).transpose(0, 2, 1).reshape(seqs * heads, length)
    log_decay_total = -head_decay_rate[None, :, None] * jax.nn.softplus(decay_logits.transpose(0, 2, 1)) + extra_log_decay.transpose(0, 2, 1)
    log_decay_total = log_decay_total.reshape(seqs * heads, length)
    attended = lax.map(run_head, (query, keyed, valued, beta, log_decay_total))
    normed = attended * lax.rsqrt(lax.optimization_barrier(jnp.mean(attended * attended, axis=-1, keepdims=True)) + eps) * head_norm_gain
    normed = normed.astype(jnp.bfloat16).reshape(seqs, heads, length, width).transpose(0, 2, 1, 3).reshape(seqs * length, joined)
    gated = (normed.astype(jnp.float32) * jax.nn.silu(output_gate_proj.reshape(seqs * length, joined).astype(jnp.float32))).astype(jnp.bfloat16)
    mixed = residual.reshape(seqs * length, model).astype(jnp.float32) + jnp.dot(gated.astype(jnp.float32), output_matrix.astype(jnp.float32), preferred_element_type=jnp.float32)
    ffn_in = (mixed * lax.rsqrt(lax.optimization_barrier(jnp.mean(mixed * mixed, axis=-1, keepdims=True)) + eps) * expert_norm_gain).astype(jnp.bfloat16)
    experts = gate_weight.shape[0]
    groups = group_router_scores.shape[-1]
    per_group = experts // groups
    chosen = routes.reshape(seqs * length, 2)
    group_exp = jnp.exp(group_router_scores.reshape(seqs * length, groups))
    group_id = chosen[:, 0] // per_group
    match = jnp.arange(groups, dtype=jnp.int32)[None, :] == group_id[:, None]
    group_prob = lax.optimization_barrier(jnp.sum(jnp.where(match, group_exp, 0.0), axis=-1)) / lax.optimization_barrier(jnp.sum(group_exp, axis=-1))
    pick_exp = jnp.exp(chosen_expert_scores.reshape(seqs * length, 2))
    weight = group_prob[:, None] * pick_exp / lax.optimization_barrier(jnp.sum(pick_exp, axis=-1, keepdims=True))
    expert_out = routed(ffn_in, chosen, gate_weight, up_weight, down_weight)
    moe = lax.optimization_barrier(jnp.sum(weight[..., None] * expert_out.astype(jnp.float32), axis=1))
    return (mixed + moe).astype(jnp.bfloat16).reshape(seqs, length, model)
```

```python
import jax
import jax.numpy as jnp
from jax import lax
from jax.experimental import pallas as pl
from jax.experimental.pallas import tpu as pltpu
from jax.sharding import PartitionSpec as P

F32 = jnp.float32
BF16 = jnp.bfloat16
MESH = pl.DeviceIdType.MESH
EPS = 1e-06
T = 128
HD = 64
NH = 16
D = 2048
HALF = D // 2
FF = 1024
NE = 128
CHUNKS = 4
PER = NE // CHUNKS


def coords():
    sp = lax.axis_index("sp")
    dp = lax.axis_index("dp")
    return sp >> 2, sp & 3, dp >> 1, dp & 1


def at(z, x, y, c):
    return (((z & 3) << 2) + (x & 3), ((y & 3) << 1) + (c & 1))


def offset(i):
    chunk = i >> 5
    dx = (i >> 3) & 3
    dy = (i >> 1) & 3
    return (chunk - dx - dy) & 3, dx, dy, i & 1


def iota(shape, dim):
    return lax.broadcasted_iota(jnp.int32, shape, dim)


def split(a):
    hi = a.astype(BF16)
    return hi, (a - hi.astype(F32)).astype(BF16)


def dot(a, b):
    return jnp.dot(a, b, preferred_element_type=F32)


def dot3(a, b):
    (ah, al), (bh, bl) = a, b
    return dot(jnp.concatenate([ah, ah, al], axis=1), jnp.concatenate([bh, bl, bh], axis=0))


def roll64(a):
    return pltpu.roll(a, 64, 1)


def kernel(
    small_ref, rate_ref, hgain_ref, egain_ref,
    q_hbm, k_hbm, v_hbm, gate_hbm, res_hbm, om_hbm, wg_hbm, wu_hbm, wd_hbm,
    out_ref,
    q_ref, k_ref, v_ref, gate_ref, res_ref, om_ref, wg_ref, wu_ref, wd_ref,
    rates, raw, kt_ref, rhs_v, rhs_k, qroll, silu_g, cols, rows_ref,
    mb_out, mb_in, s_out, s_in, oloc, pbuf, gated, mixed, x2,
    sel, wsel, out_buf, arrived, prod, back, xs, acc,
    load_sem, rate_sem, mb_sem, s_sem, fwd_send, fwd_recv, ret_send, ret_recv, all_in,
):
    z, x, y, c = coords()
    sp = (z << 2) + x
    partner = at(z, x, y, c + 1)

    loads = [
        pltpu.make_async_copy(src, dst, load_sem.at[i])
        for i, (src, dst) in enumerate(
            (
                (k_hbm, k_ref), (q_hbm, q_ref), (v_hbm, v_ref), (gate_hbm, gate_ref),
                (res_hbm, res_ref), (om_hbm, om_ref),
                (wg_hbm, wg_ref), (wu_hbm, wu_ref), (wd_hbm, wd_ref),
            )
        )
    ]
    for copy in loads:
        copy.start()

    barrier = pltpu.get_barrier_semaphore()

    def greet_sp(i, carry):
        pl.semaphore_signal(barrier, 1, device_id=at(z + (i >> 2), x + i, y, c), device_id_type=MESH)
        return carry

    def greet_dp(i, carry):
        pl.semaphore_signal(barrier, 1, device_id=at(z, x, y + (i >> 1), c + i), device_id_type=MESH)
        return carry

    lax.fori_loop(1, 16, greet_sp, 0)
    lax.fori_loop(1, 8, greet_dp, 0)

    def many_recv(buf, count, sem):
        part = buf.at[pl.ds(0, count)]
        pltpu.make_async_remote_copy(part, part, sem, sem, device_id=partner, device_id_type=MESH).wait_recv()

    def many_sent(buf, count, sem):
        part = buf.at[pl.ds(0, count)]
        pltpu.make_async_remote_copy(part, part, sem, sem, device_id=partner, device_id_type=MESH).wait_send()

    lane = iota((T, T), 1)
    sub = iota((T, T), 0)
    low_half = lane < HD

    small = small_ref[...]
    e0 = small[:, 54:55].astype(jnp.int32)
    e1 = small[:, 55:56].astype(jnp.int32)
    one0 = jnp.where(lane == e0, 1.0, 0.0)
    one1 = jnp.where(lane == e1, 1.0, 0.0)
    before = dot(jnp.where(sub > lane, 1.0, 0.0).astype(BF16), (one0 + one1).astype(BF16))
    rank0 = jnp.sum(before * one0, axis=1, keepdims=True).astype(jnp.int32)
    rank1 = jnp.sum(before * one1, axis=1, keepdims=True).astype(jnp.int32)

    def slot_of(e, rank):
        dz = ((e >> 5) - z) & 3
        dx = ((e >> 3) - x) & 3
        dy = ((e >> 1) - y) & 3
        dc = (e - c) & 1
        return ((((dz + dx + dy) & 3) << 5) + (dx << 3) + (dy << 1) + dc) * 8 + rank

    slot0 = slot_of(e0, rank0)
    slot1 = slot_of(e1, rank1)
    scores = jnp.exp(small)
    is_group = (lane >= 48) & (lane < 52)
    is_pick = (lane >= 52) & (lane < 54)
    own_group = lane == (e0 >> 5) + 48
    group_sum = jnp.sum(jnp.where(is_group, scores, 0.0), axis=1, keepdims=True)
    group_own = jnp.sum(jnp.where(own_group, scores, 0.0), axis=1, keepdims=True)
    pick_sum = jnp.sum(jnp.where(is_pick, scores, 0.0), axis=1, keepdims=True)
    prob = group_own / group_sum
    w0 = prob * scores[:, 52:53] / pick_sum
    w1 = prob * scores[:, 53:54] / pick_sum
    wide = iota((T, NE * 8), 1)
    for h in range(2):
        w = jnp.where(wide == slot0 + 4 * h, w0, 0.0) + jnp.where(wide == slot1 + 4 * h, w1, 0.0)
        hi, lo = split(w)
        wsel[h * T : (h + 1) * T, :] = hi
        wsel[(2 + h) * T : (3 + h) * T, :] = lo
    slot_cols = jnp.where(lane == 0, slot0.astype(F32), slot1.astype(F32))
    slot_rows = jnp.transpose(slot_cols)
    row0 = slot_rows[0:1, :].astype(jnp.int32)
    row1 = slot_rows[1:2, :].astype(jnp.int32)
    tall = iota((NE * 8, T), 0)
    for h in range(2):
        hit = (tall == row0 + 4 * h) | (tall == row1 + 4 * h)
        sel[:, h * T : (h + 1) * T] = jnp.where(hit, 1.0, 0.0).astype(BF16)

    loads[0].wait()
    loads[1].wait()
    loads[2].wait()
    sums = jnp.zeros((2 * T, T), F32)
    sel_row = iota((2 * T, T), 0)
    sel_lane = iota((2 * T, T), 1)
    sel_head = (sel_row & 127) >> 6
    for j in range(NH // 2):
        cut = slice(j * T, (j + 1) * T)
        kb = k_ref[:, cut]
        qb = q_ref[:, cut]
        k32 = kb.astype(F32)
        q32 = qb.astype(F32)
        hi, lo = split(jnp.concatenate([k32 * k32, q32 * q32], axis=0))
        pick = jnp.where(sel_lane == sel_head + 2 * j, 1.0, 0.0).astype(BF16)
        sums = sums + dot(jnp.concatenate([hi, lo], axis=1), pick)
        kt = jnp.transpose(k32)
        kt_ref[j] = kt
        both = jnp.concatenate(
            [jnp.where(sub < HD, kt, 0.0), jnp.where(sub < HD, 0.0, kt)], axis=1
        ).astype(BF16)
        prods = dot(jnp.concatenate([kb, qb], axis=0), both)
        raw[2 * j] = prods[:, :T]
        raw[2 * j + 1] = prods[:, T:]
        v32 = v_ref[:, cut].astype(F32)
        kr = roll64(k32)
        rhs_v[2 * j] = jnp.where(low_half, v32, 0.0).astype(BF16)
        rhs_v[2 * j + 1] = jnp.where(low_half, 0.0, v32).astype(BF16)
        rhs_k[2 * j] = jnp.where(low_half, 0.0, kr).astype(BF16)
        rhs_k[2 * j + 1] = jnp.where(low_half, kr, 0.0).astype(BF16)
        qroll[j] = roll64(q32)
    inv = lax.rsqrt(sums + EPS)
    rk = inv[:T]
    rq = inv[T:] * (HD**-0.5)
    loads[3].wait()
    for j in range(NH // 2):
        cut = slice(j * T, (j + 1) * T)
        v32 = gate_ref[:, cut].astype(F32)
        silu_g[:, cut] = v32 / (1.0 + jnp.exp(-v32))

    pl.semaphore_wait(barrier, 22)

    def send_rate(i, carry):
        pltpu.make_async_remote_copy(
            rate_ref, rates.at[sp], rate_sem.at[0], rate_sem.at[1],
            device_id=at(z + (i >> 2), x + i, y, c), device_id_type=MESH,
        ).start()
        return carry

    lax.fori_loop(1, 16, send_rate, 0)

    def tell_in(i, carry):
        pl.semaphore_signal(all_in, 1, device_id=at(z, x, y + (i >> 1), c + i), device_id_type=MESH)
        return carry

    lax.fori_loop(1, 8, tell_in, 0)
    rates[sp] = rate_ref[...]
    is_head = lane < NH
    beta = jax.nn.sigmoid(jnp.where(is_head, small, 0.0))
    dl = jnp.where(is_head, pltpu.roll(small, T - 16, 1), 0.0)
    el = jnp.where(is_head, pltpu.roll(small, T - 32, 1), 0.0)
    soft = jax.nn.softplus(dl)
    many_recv(rates, 15, rate_sem.at[1])
    eye16 = iota((NH, T), 0) == iota((NH, T), 1)
    rate_row = jnp.sum(jnp.where(eye16, rates[:, 0, :], 0.0), axis=0, keepdims=True)
    g = jnp.where(is_head, el - rate_row * soft, 0.0)
    g1 = g.astype(BF16)
    rest = g - g1.astype(F32)
    g2, g3 = split(rest)
    tri = jnp.where(sub >= lane, 1.0, 0.0).astype(BF16)
    cumul = dot(jnp.concatenate([tri, tri, tri], axis=1), jnp.concatenate([g1, g2, g3], axis=0))
    packed = (
        jnp.where(is_head, cumul, 0.0)
        + pltpu.roll(jnp.where(is_head, rk, 0.0), 16, 1)
        + pltpu.roll(jnp.where(is_head, beta, 0.0), 32, 1)
        + pltpu.roll(jnp.where(is_head, rq, 0.0), 48, 1)
    )
    rows_ref[...] = jnp.transpose(packed)
    colpack = (
        jnp.where(is_head, cumul, 0.0)
        + pltpu.roll(jnp.where(is_head, beta * rk, 0.0), 16, 1)
        + pltpu.roll(jnp.where(is_head, rq, 0.0), 32, 1)
    )
    cols[0] = colpack
    for n in range(1, 4):
        cols[n] = pltpu.roll(colpack, T - 4 * n, 1)

    def heads(n, carry):
        col = cols.at[n]
        causal = sub >= lane
        ls, atts, ups, ws, kds, tots = [], [], [], [], [], []
        for hh in range(4):
            h = n * 4 + hh
            c_row = rows_ref[pl.ds(h, 1), :]
            k_row = rows_ref[pl.ds(h + 16, 1), :]
            b_row = rows_ref[pl.ds(h + 32, 1), :]
            c_col = col[:, hh : hh + 1]
            dec = jnp.where(causal, jnp.exp(jnp.minimum(c_col - c_row, 0.0)), 0.0) * k_row
            ls.append(jnp.where(sub > lane, raw[h, 0:T, :] * dec * col[:, hh + 16 : hh + 17], 0.0))
            atts.append(raw[h, T : 2 * T, :] * dec * col[:, hh + 32 : hh + 33])
            ups.append(b_row)
            ws.append(b_row * k_row * jnp.exp(c_row))
            last = c_row[:, T - 1 : T]
            kds.append(k_row * jnp.exp(last - c_row))
            tots.append(jnp.exp(last))
        pairs = sub >> 1 == lane >> 1
        ts = [jnp.where(sub == lane, 1.0, 0.0) - jnp.where(pairs, l, 0.0) for l in ls]
        for bits in range(1, 7):
            m = ((sub >> bits) == (lane >> bits) + 1) & (((sub >> bits) & 1) == 1)
            tsp = [split(t) for t in ts]
            xsp = [split(dot3(split(jnp.where(m, l, 0.0)), t)) for l, t in zip(ls, tsp)]
            ts = [t - dot3(tp, xx) for t, tp, xx in zip(ts, tsp, xsp)]
        auws = []
        for hh in range(4):
            h = n * 4 + hh
            uh, ul = split(ts[hh] * ups[hh])
            wh, wl = split(ts[hh] * ws[hh])
            vm = rhs_v[h]
            km = rhs_k[h]
            uw = dot(jnp.concatenate([uh, ul, wh, wl], axis=1), jnp.concatenate([vm, vm, km, km], axis=0))
            ktp = kt_ref[n * 2 + hh // 2, (hh % 2) * HD : (hh % 2) * HD + HD, :]
            both = jnp.concatenate([atts[hh], ktp * kds[hh]], axis=0)
            res = dot3(split(both), split(uw))
            auws.append(res[:T])
            bn = res[T:]
            if hh % 2:
                bn = roll64(bn)
            lane64 = iota((HD, T), 1)
            ident = jnp.where(lane64 - HD == iota((HD, T), 0), tots[hh], 0.0)
            mb_out[h] = jnp.where(lane64 < HD, bn, ident - bn)
        for jj in range(2):
            j = n * 2 + jj
            a, b = 2 * jj, 2 * jj + 1
            sc_a = col[:, a + 32 : a + 33] * jnp.exp(col[:, a : a + 1])
            sc_b = col[:, b + 32 : b + 33] * jnp.exp(col[:, b : b + 1])
            p = qroll[j] * jnp.where(low_half, sc_b, sc_a) - jnp.where(low_half, auws[b], auws[a])
            hi, lo = split(p)
            pbuf[j, :, 0:T] = hi
            pbuf[j, :, T : 2 * T] = lo
            oloc[j] = jnp.where(low_half, auws[a], auws[b])
        for hh in range(4):
            h = n * 4 + hh

            @pl.when(h == sp)
            def _():
                mb_in[h] = mb_out[h]

            @pl.when(h != sp)
            def _():
                pltpu.make_async_remote_copy(
                    mb_out.at[h], mb_in.at[sp], mb_sem.at[0], mb_sem.at[1],
                    device_id=at(n, hh, y, c), device_id_type=MESH,
                ).start()

        return carry

    lax.fori_loop(0, 4, heads, 0)

    many_recv(mb_in, 15, mb_sem.at[1])
    lane64 = iota((HD, T), 1)
    sub64 = iota((HD, T), 0)
    ident = jnp.where((lane64 & 63) == sub64, 1.0, 0.0).astype(BF16)
    mine = (lane64 >> 6) == (sp & 1)
    zero = jnp.zeros((HD, T), BF16)
    place = sp + 1 - 2 * (sp & 1)
    state = jnp.zeros((HD, T), F32)
    for p in range(16):
        s_out[p] = jnp.where(mine, state, 0.0).astype(BF16)

        @pl.when(sp == p)
        def _():
            s_in[place] = s_out[p]

        @pl.when(sp != p)
        def _():
            pltpu.make_async_remote_copy(
                s_out.at[p], s_in.at[place], s_sem.at[0], s_sem.at[1],
                device_id=at(p >> 2, p, y, c), device_id_type=MESH,
            ).start()

        if p < 15:
            sh, sl = split(state)
            state = dot3(
                split(mb_in[p]),
                (jnp.concatenate([ident, sh], axis=0), jnp.concatenate([zero, sl], axis=0)),
            )

    many_recv(s_in, 15, s_sem.at[1])
    ones = jnp.where((iota((2 * T, T), 0) >> 6) & 1 == iota((2 * T, T), 1) >> 6, 1.0, 0.0).astype(BF16)
    for j in range(NH // 2):
        cut = slice(j * T, (j + 1) * T)
        sj = s_in[2 * j : 2 * j + 2].reshape(T, T)
        o = oloc[j] + dot(pbuf[j], jnp.concatenate([sj, sj], axis=0))
        hi, lo = split(o * o)
        mean = dot(jnp.concatenate([hi, lo], axis=1), ones) * (1.0 / HD)
        normed = (o * lax.rsqrt(mean + EPS) * hgain_ref[...]).astype(BF16)
        gated[:, cut] = (normed.astype(F32) * silu_g[:, cut]).astype(BF16)
    loads[4].wait()
    loads[5].wait()
    total = jnp.zeros((T, 1), F32)
    for n in range(4):
        cut = slice(n * 512, (n + 1) * 512)
        m = res_ref[:, cut].astype(F32) + dot(gated[...], om_ref[:, cut])
        mixed[:, cut] = m
        total = total + jnp.sum(m * m, axis=1, keepdims=True)
    inv = lax.rsqrt(total * (1.0 / D) + EPS)
    for h in range(2):
        cut = slice(h * HALF, (h + 1) * HALF)
        x2[h * T : (h + 1) * T, :] = (mixed[:, cut] * inv * egain_ref[:, cut]).astype(BF16)

    pl.semaphore_wait(all_in, 7)

    def dispatch(n, carry):
        block = dot(sel[pl.ds(n * 256, 256), :], x2[...]).astype(BF16)
        out_buf[pl.ds(n * PER, PER)] = block.reshape(PER, 8, HALF)

        def send(j, inner):
            i = n * PER + j
            dz, dx, dy, dc = offset(i)

            @pl.when(i != 0)
            def _():
                pltpu.make_async_remote_copy(
                    out_buf.at[i], arrived.at[i], fwd_send, fwd_recv.at[n],
                    device_id=at(z + dz, x + dx, y + dy, c + dc), device_id_type=MESH,
                ).start()

            return inner

        lax.fori_loop(0, PER, send, 0)
        return carry

    lax.fori_loop(0, CHUNKS, dispatch, 0)
    arrived[0] = out_buf[0]
    loads[6].wait()
    loads[7].wait()
    loads[8].wait()

    sub256 = iota((256, 256), 0)
    lane256 = iota((256, 256), 1)
    source = ((sub256 & 127) >> 2) * 8 + (sub256 >> 7) * 4 + (sub256 & 3)
    apart = jnp.where(source == lane256, 1.0, 0.0).astype(BF16)
    source = ((lane256 & 127) >> 2) * 8 + (lane256 >> 7) * 4 + (lane256 & 3)
    together = jnp.where(source == sub256, 1.0, 0.0).astype(BF16)

    def expert(n, carry):
        @pl.when(n == 0)
        def _():
            many_recv(arrived, PER - 1, fwd_recv.at[0])

        @pl.when(n != 0)
        def _():
            many_recv(arrived, PER, fwd_recv.at[n])

        rows = arrived[pl.ds(n * PER, PER)].reshape(256, HALF)
        xs[...] = dot(apart, rows).astype(BF16)
        for k in range(4):
            cut = slice(k * 256, (k + 1) * 256)
            gate = dot(xs[0:T, :], wg_ref[0:HALF, cut]) + dot(xs[T : 2 * T, :], wg_ref[HALF:D, cut])
            upper = dot(xs[0:T, :], wu_ref[0:HALF, cut]) + dot(xs[T : 2 * T, :], wu_ref[HALF:D, cut])
            acc[:, cut] = (gate / (1.0 + jnp.exp(-gate)) * upper).astype(BF16)
        for k in range(8):
            cut = slice(k * 256, (k + 1) * 256)
            half, inside = k // 4, slice((k % 4) * 256, (k % 4 + 1) * 256)
            xs[half * T : (half + 1) * T, inside] = dot(acc[...], wd_ref[:, cut]).astype(BF16)
        prod[pl.ds(n * PER, PER)] = dot(together, xs[...]).astype(BF16).reshape(PER, 8, HALF)

        def send(j, inner):
            i = n * PER + j
            dz, dx, dy, dc = offset(i)

            @pl.when(i != 0)
            def _():
                pltpu.make_async_remote_copy(
                    prod.at[i], back.at[i], ret_send, ret_recv.at[n],
                    device_id=at(z - dz, x - dx, y - dy, c - dc), device_id_type=MESH,
                ).start()

            return inner

        lax.fori_loop(0, PER, send, 0)
        return carry

    lax.fori_loop(0, CHUNKS, expert, 0)
    back[0] = prod[0]

    for n in range(CHUNKS):
        many_recv(back, PER - 1 if n == 0 else PER, ret_recv.at[n])
        part = dot(wsel[:, n * 256 : (n + 1) * 256], back[n * PER : (n + 1) * PER].reshape(256, HALF))
        for h in range(2):
            cut = slice(h * HALF, (h + 1) * HALF)
            total = mixed[:, cut] + (part[h * T : (h + 1) * T] + part[(2 + h) * T : (3 + h) * T])
            if n < CHUNKS - 1:
                mixed[:, cut] = total
            else:
                out_ref[:, cut] = total.astype(BF16)

    many_sent(rates, 15, rate_sem.at[0])
    many_sent(mb_out, 15, mb_sem.at[0])
    many_sent(s_out, 15, s_sem.at[0])
    many_sent(out_buf, NE - 1, fwd_send)
    many_sent(prod, NE - 1, ret_send)


def call(small, rate, hgain, egain, *big):
    vm = pl.BlockSpec(memory_space=pltpu.VMEM)
    hbm = pl.BlockSpec(memory_space=pl.ANY)
    return pl.pallas_call(
        kernel,
        out_shape=jax.ShapeDtypeStruct((T, D), BF16),
        in_specs=[vm] * 4 + [hbm] * 9,
        out_specs=vm,
        scratch_shapes=[
            pltpu.VMEM((T, NH * HD), BF16),
            pltpu.VMEM((T, NH * HD), BF16),
            pltpu.VMEM((T, NH * HD), BF16),
            pltpu.VMEM((T, NH * HD), BF16),
            pltpu.VMEM((T, D), BF16),
            pltpu.VMEM((NH * HD, D), BF16),
            pltpu.VMEM((D, FF), BF16),
            pltpu.VMEM((D, FF), BF16),
            pltpu.VMEM((FF, D), BF16),
            pltpu.VMEM((16, 8, T), F32),
            pltpu.VMEM((NH, 2 * T, T), F32),
            pltpu.VMEM((NH // 2, T, T), F32),
            pltpu.VMEM((NH, T, T), BF16),
            pltpu.VMEM((NH, T, T), BF16),
            pltpu.VMEM((NH // 2, T, T), F32),
            pltpu.VMEM((T, NH * HD), F32),
            pltpu.VMEM((4, T, T), F32),
            pltpu.VMEM((T, T), F32),
            pltpu.VMEM((NH, HD, T), F32),
            pltpu.VMEM((NH, HD, T), F32),
            pltpu.VMEM((NH, HD, T), BF16),
            pltpu.VMEM((NH, HD, T), BF16),
            pltpu.VMEM((NH // 2, T, T), F32),
            pltpu.VMEM((NH // 2, T, 2 * T), BF16),
            pltpu.VMEM((T, NH * HD), BF16),
            pltpu.VMEM((T, D), F32),
            pltpu.VMEM((2 * T, HALF), BF16),
            pltpu.VMEM((NE * 8, 2 * T), BF16),
            pltpu.VMEM((4 * T, NE * 8), BF16),
            pltpu.VMEM((NE, 8, HALF), BF16),
            pltpu.VMEM((NE, 8, HALF), BF16),
            pltpu.VMEM((NE, 8, HALF), BF16),
            pltpu.VMEM((NE, 8, HALF), BF16),
            pltpu.VMEM((2 * T, HALF), BF16),
            pltpu.VMEM((T, FF), BF16),
            pltpu.SemaphoreType.DMA((9,)),
            pltpu.SemaphoreType.DMA((2,)),
            pltpu.SemaphoreType.DMA((2,)),
            pltpu.SemaphoreType.DMA((2,)),
            pltpu.SemaphoreType.DMA,
            pltpu.SemaphoreType.DMA((CHUNKS,)),
            pltpu.SemaphoreType.DMA,
            pltpu.SemaphoreType.DMA((CHUNKS,)),
            pltpu.SemaphoreType.REGULAR,
        ],
        compiler_params=pltpu.CompilerParams(
            collective_id=0, has_side_effects=True, vmem_limit_bytes=60 * 1024 * 1024
        ),
        name="layer",
    )(small, rate, hgain, egain, *big)


def shards(
    residual, query, key, value, output_gate, write_logits, decay_logits, extra_decay, head_rate,
    head_gain, output_matrix, expert_gain, group_scores, expert_scores, routes,
    gate_weight, up_weight, down_weight,
):
    small = jnp.concatenate(
        [
            write_logits[0], decay_logits[0], extra_decay[0], group_scores[0], expert_scores[0],
            routes[0].astype(F32), jnp.zeros((T, T - 56), F32),
        ],
        axis=1,
    )
    rate = jnp.broadcast_to(head_rate[:, None], (8, T))
    hgain = jnp.tile(head_gain, 2)[None]
    out = call(
        small, rate, hgain, expert_gain[None], query[0], key[0], value[0], output_gate[0],
        residual[0], output_matrix, gate_weight[0], up_weight[0], down_weight[0],
    )
    return out[None]


def solution(mesh):
    tok = P("dp", "sp", None)
    exp = P(("sp", "dp"), None, None)
    in_specs = (
        (tok,) * 8 + (P("sp"), P(), P(), P()) + (tok,) * 3 + (exp,) * 3
    )
    return jax.shard_map(shards, mesh=mesh, in_specs=in_specs, out_specs=tok, check_vma=False)
```

```python
import jax
import jax.numpy as jnp
from jax import lax
from jax.experimental import pallas as pl
from jax.experimental.pallas import tpu as pltpu
from jax.sharding import PartitionSpec as P

F32 = jnp.float32
BF16 = jnp.bfloat16
MESH = pl.DeviceIdType.MESH
EPS = 1e-06
T = 128
HD = 64
NH = 16
D = 2048
HALF = D // 2
FF = 1024
NE = 128
CHUNKS = 4
PER = NE // CHUNKS


def coords():
    sp = lax.axis_index("sp")
    dp = lax.axis_index("dp")
    return sp >> 2, sp & 3, dp >> 1, dp & 1


def at(z, x, y, c):
    return (((z & 3) << 2) + (x & 3), ((y & 3) << 1) + (c & 1))


def offset(i):
    chunk = i >> 5
    dx = (i >> 3) & 3
    dy = (i >> 1) & 3
    return (chunk - dx - dy) & 3, dx, dy, i & 1


def iota(shape, dim):
    return lax.broadcasted_iota(jnp.int32, shape, dim)


def split(a):
    hi = a.astype(BF16)
    return hi, (a - hi.astype(F32)).astype(BF16)


def dot(a, b):
    return jnp.dot(a, b, preferred_element_type=F32)


def dot3(a, b):
    (ah, al), (bh, bl) = a, b
    return dot(jnp.concatenate([ah, ah, al], axis=1), jnp.concatenate([bh, bl, bh], axis=0))


def dot4(a, b):
    (ah, al), (bh, bl) = a, b
    left = jnp.concatenate(
        [jnp.concatenate([ah, ah], axis=1), jnp.concatenate([al, al], axis=1)], axis=0
    )
    both = dot(left, jnp.concatenate([bh, bl], axis=0))
    return both[: ah.shape[0]] + both[ah.shape[0] :]


def odd_blocks(a, size):
    return jnp.concatenate([a[i : i + size] for i in range(size, T, 2 * size)], axis=0)


def with_odd_blocks(even, odd, size):
    parts = []
    for n, i in enumerate(range(0, T, 2 * size)):
        parts += [even[i : i + size], odd[n * size : (n + 1) * size]]
    return jnp.concatenate(parts, axis=0)


def roll64(a):
    return pltpu.roll(a, 64, 1)


def kernel(
    wsl_ref, dl_ref, el_ref, grs_ref, ces_ref, routes_ref, rate_in, hg_ref, egain_ref,
    q_hbm, k_hbm, v_hbm, gate_hbm, res_hbm, om_hbm, wg_hbm, wu_hbm, wd_hbm,
    out_ref,
    q_ref, k_ref, v_ref, gate_ref, res_ref, om_ref, wg_ref, wu_ref, wd_ref,
    small_rows, rate_ref, hgain_ref, rates, raw, kt_ref, rhs_v, rhs_k, qroll, silu_g, cols, rows_ref,
    uwbuf, mb_out, mb_in, s_out, s_in, oloc, pbuf, gated, mixed, x2,
    sel, wsel, out_buf, arrived, prod, back, xs, acc,
    load_sem, rate_sem, mb_sem, s_sem, fwd_send, fwd_recv, ret_send, ret_recv, all_in,
):
    z, x, y, c = coords()
    sp = (z << 2) + x
    partner = at(z, x, y, c + 1)

    loads = [
        pltpu.make_async_copy(src, dst, load_sem.at[i])
        for i, (src, dst) in enumerate(
            (
                (k_hbm, k_ref), (q_hbm, q_ref), (v_hbm, v_ref), (gate_hbm, gate_ref),
                (res_hbm, res_ref), (om_hbm, om_ref),
                (wg_hbm, wg_ref), (wu_hbm, wu_ref), (wd_hbm, wd_ref),
            )
        )
    ]
    for copy in loads:
        copy.start()

    barrier = pltpu.get_barrier_semaphore()

    def greet_sp(i, carry):
        pl.semaphore_signal(barrier, 1, device_id=at(z + (i >> 2), x + i, y, c), device_id_type=MESH)
        return carry

    def greet_dp(i, carry):
        pl.semaphore_signal(barrier, 1, device_id=at(z, x, y + (i >> 1), c + i), device_id_type=MESH)
        return carry

    lax.fori_loop(1, 16, greet_sp, 0)
    lax.fori_loop(1, 8, greet_dp, 0)

    def many_recv(buf, count, sem):
        part = buf.at[pl.ds(0, count)]
        pltpu.make_async_remote_copy(part, part, sem, sem, device_id=partner, device_id_type=MESH).wait_recv()

    def many_sent(buf, count, sem):
        part = buf.at[pl.ds(0, count)]
        pltpu.make_async_remote_copy(part, part, sem, sem, device_id=partner, device_id_type=MESH).wait_send()

    lane = iota((T, T), 1)
    sub = iota((T, T), 0)
    low_half = lane < HD

    rate_ref[...] = jnp.full((8, T), rate_in[0], F32)
    hgain_ref[:, 0:HD] = hg_ref[...]
    hgain_ref[:, HD:T] = hg_ref[...]
    small_rows[...] = jnp.zeros((T, T), F32)
    small_rows[0:16, :] = wsl_ref[...]
    small_rows[16:32, :] = dl_ref[...]
    small_rows[32:48, :] = el_ref[...]
    small_rows[48:52, :] = grs_ref[...]
    small_rows[52:54, :] = ces_ref[...]
    small_rows[54:56, :] = routes_ref[...].astype(F32)
    small = jnp.transpose(small_rows[...])
    e0 = small[:, 54:55].astype(jnp.int32)
    e1 = small[:, 55:56].astype(jnp.int32)
    one0 = jnp.where(lane == e0, 1.0, 0.0)
    one1 = jnp.where(lane == e1, 1.0, 0.0)
    before = dot(jnp.where(sub > lane, 1.0, 0.0).astype(BF16), (one0 + one1).astype(BF16))
    rank0 = jnp.sum(before * one0, axis=1, keepdims=True).astype(jnp.int32)
    rank1 = jnp.sum(before * one1, axis=1, keepdims=True).astype(jnp.int32)

    def slot_of(e, rank):
        dz = ((e >> 5) - z) & 3
        dx = ((e >> 3) - x) & 3
        dy = ((e >> 1) - y) & 3
        dc = (e - c) & 1
        return ((((dz + dx + dy) & 3) << 5) + (dx << 3) + (dy << 1) + dc) * 8 + rank

    slot0 = slot_of(e0, rank0)
    slot1 = slot_of(e1, rank1)
    scores = jnp.exp(small)
    is_group = (lane >= 48) & (lane < 52)
    is_pick = (lane >= 52) & (lane < 54)
    own_group = lane == (e0 >> 5) + 48
    group_sum = jnp.sum(jnp.where(is_group, scores, 0.0), axis=1, keepdims=True)
    group_own = jnp.sum(jnp.where(own_group, scores, 0.0), axis=1, keepdims=True)
    pick_sum = jnp.sum(jnp.where(is_pick, scores, 0.0), axis=1, keepdims=True)
    prob = group_own / group_sum
    w0 = prob * scores[:, 52:53] / pick_sum
    w1 = prob * scores[:, 53:54] / pick_sum
    wide = iota((T, NE * 8), 1)
    for h in range(2):
        w = jnp.where(wide == slot0 + 4 * h, w0, 0.0) + jnp.where(wide == slot1 + 4 * h, w1, 0.0)
        hi, lo = split(w)
        wsel[h * T : (h + 1) * T, :] = hi
        wsel[(2 + h) * T : (3 + h) * T, :] = lo
    slot_cols = jnp.where(lane == 0, slot0.astype(F32), slot1.astype(F32))
    slot_rows = jnp.transpose(slot_cols)
    row0 = slot_rows[0:1, :].astype(jnp.int32)
    row1 = slot_rows[1:2, :].astype(jnp.int32)
    tall = iota((NE * 8, T), 0)
    for h in range(2):
        hit = (tall == row0 + 4 * h) | (tall == row1 + 4 * h)
        sel[:, h * T : (h + 1) * T] = jnp.where(hit, 1.0, 0.0).astype(BF16)

    loads[0].wait()
    loads[1].wait()
    loads[2].wait()
    sums = jnp.zeros((2 * T, T), F32)
    sel_row = iota((2 * T, T), 0)
    sel_lane = iota((2 * T, T), 1)
    sel_head = (sel_row & 127) >> 6
    for j in range(NH // 2):
        cut = slice(j * T, (j + 1) * T)
        kb = k_ref[:, cut]
        qb = q_ref[:, cut]
        k32 = kb.astype(F32)
        q32 = qb.astype(F32)
        hi, lo = split(jnp.concatenate([k32 * k32, q32 * q32], axis=0))
        pick = jnp.where(sel_lane == sel_head + 2 * j, 1.0, 0.0).astype(BF16)
        sums = sums + dot(jnp.concatenate([hi, lo], axis=1), pick)
        kt = jnp.transpose(k32)
        kt_ref[j] = kt
        both = jnp.concatenate(
            [jnp.where(sub < HD, kt, 0.0), jnp.where(sub < HD, 0.0, kt)], axis=1
        ).astype(BF16)
        prods = dot(jnp.concatenate([kb, qb], axis=0), both)
        raw[2 * j] = prods[:, :T]
        raw[2 * j + 1] = prods[:, T:]
        v32 = v_ref[:, cut].astype(F32)
        kr = roll64(k32)
        rhs_v[2 * j] = jnp.where(low_half, v32, 0.0).astype(BF16)
        rhs_v[2 * j + 1] = jnp.where(low_half, 0.0, v32).astype(BF16)
        rhs_k[2 * j] = jnp.where(low_half, 0.0, kr).astype(BF16)
        rhs_k[2 * j + 1] = jnp.where(low_half, kr, 0.0).astype(BF16)
        qroll[j] = roll64(q32)
    inv = lax.rsqrt(sums + EPS)
    rk = inv[:T]
    rq = inv[T:] * (HD**-0.5)
    loads[3].wait()
    for j in range(NH // 2):
        cut = slice(j * T, (j + 1) * T)
        v32 = gate_ref[:, cut].astype(F32)
        silu_g[:, cut] = v32 / (1.0 + jnp.exp(-v32))

    pl.semaphore_wait(barrier, 22)

    def send_rate(i, carry):
        pltpu.make_async_remote_copy(
            rate_ref, rates.at[sp], rate_sem.at[0], rate_sem.at[1],
            device_id=at(z + (i >> 2), x + i, y, c), device_id_type=MESH,
        ).start()
        return carry

    lax.fori_loop(1, 16, send_rate, 0)

    def tell_in(i, carry):
        pl.semaphore_signal(all_in, 1, device_id=at(z, x, y + (i >> 1), c + i), device_id_type=MESH)
        return carry

    lax.fori_loop(1, 8, tell_in, 0)
    rates[sp] = rate_ref[...]
    is_head = lane < NH
    beta = jax.nn.sigmoid(jnp.where(is_head, small, 0.0))
    dl = jnp.where(is_head, pltpu.roll(small, T - 16, 1), 0.0)
    el = jnp.where(is_head, pltpu.roll(small, T - 32, 1), 0.0)
    soft = jax.nn.softplus(dl)
    many_recv(rates, 15, rate_sem.at[1])
    eye16 = iota((NH, T), 0) == iota((NH, T), 1)
    rate_row = jnp.sum(jnp.where(eye16, rates[:, 0, :], 0.0), axis=0, keepdims=True)
    g = jnp.where(is_head, el - rate_row * soft, 0.0)
    g1 = g.astype(BF16)
    rest = g - g1.astype(F32)
    g2, g3 = split(rest)
    tri = jnp.where(sub >= lane, 1.0, 0.0).astype(BF16)
    cumul = dot(jnp.concatenate([tri, tri, tri], axis=1), jnp.concatenate([g1, g2, g3], axis=0))
    packed = (
        jnp.where(is_head, cumul, 0.0)
        + pltpu.roll(jnp.where(is_head, rk, 0.0), 16, 1)
        + pltpu.roll(jnp.where(is_head, beta, 0.0), 32, 1)
        + pltpu.roll(jnp.where(is_head, rq, 0.0), 48, 1)
    )
    rows_ref[...] = jnp.transpose(packed)
    colpack = (
        jnp.where(is_head, cumul, 0.0)
        + pltpu.roll(jnp.where(is_head, beta * rk, 0.0), 16, 1)
        + pltpu.roll(jnp.where(is_head, rq, 0.0), 32, 1)
    )
    cols[0] = colpack
    for n in range(1, 4):
        cols[n] = pltpu.roll(colpack, T - 4 * n, 1)

    lane64 = iota((HD, T), 1)
    sub64 = iota((HD, T), 0)

    def heads(step, carry):
        n = (z + 3 - step) & 3
        col = cols.at[n]
        causal = sub >= lane
        ls, ups, ws, kds, tots = [], [], [], [], []
        for hh in range(4):
            h = n * 4 + hh
            c_row = rows_ref[pl.ds(h, 1), :]
            k_row = rows_ref[pl.ds(h + 16, 1), :]
            b_row = rows_ref[pl.ds(h + 32, 1), :]
            c_col = col[:, hh : hh + 1]
            dec = jnp.where(causal, jnp.exp(jnp.minimum(c_col - c_row, 0.0)), 0.0) * k_row
            ls.append(jnp.where(sub > lane, raw[h, 0:T, :] * dec * col[:, hh + 16 : hh + 17], 0.0))
            raw[h, T : 2 * T, :] = raw[h, T : 2 * T, :] * dec * col[:, hh + 32 : hh + 33]
            ups.append(b_row)
            ws.append(b_row * k_row * jnp.exp(c_row))
            last = c_row[:, T - 1 : T]
            kds.append(k_row * jnp.exp(last - c_row))
            tots.append(jnp.exp(last))
        ts = []
        pairs = (sub >> 1) == (lane >> 1)
        m = ((sub >> 1) == (lane >> 1) + 1) & (((sub >> 1) & 1) == 1)
        for l in ls:
            near = jnp.where(pairs, l, 0.0)
            far = jnp.where(m, l, 0.0)
            far = far - pltpu.roll(far, T - 1, 1) * jnp.sum(near, axis=0, keepdims=True)
            far = far - pltpu.roll(far, 1, 0) * jnp.sum(near, axis=1, keepdims=True)
            ts.append(jnp.where(sub == lane, 1.0, 0.0) - near - far)
        m = ((sub >> 2) == (lane >> 2) + 1) & (((sub >> 2) & 1) == 1)
        tsp = [split(t) for t in ts]
        xsp = [split(dot3(split(jnp.where(m, l, 0.0)), t)) for l, t in zip(ls, tsp)]
        ts = [t - dot3(tp, xx) for t, tp, xx in zip(ts, tsp, xsp)]
        for bits in range(3, 7):
            size = 1 << bits
            m = (lane64 >> bits) == 2 * (sub64 >> bits)
            none = jnp.zeros((T, T), F32)
            xs_ = [dot4(split(jnp.where(m, odd_blocks(l, size), 0.0)), split(t)) for l, t in zip(ls, ts)]
            odd = [odd_blocks(t, size) for t in ts]
            ys_ = [dot4(split(o), split(with_odd_blocks(none, x_, size))) for o, x_ in zip(odd, xs_)]
            ts = [with_odd_blocks(t, o - y_, size) for t, o, y_ in zip(ts, odd, ys_)]
        uws = []
        for hh in range(4):
            h = n * 4 + hh
            uh, ul = split(ts[hh] * ups[hh])
            wh, wl = split(ts[hh] * ws[hh])
            vm = rhs_v[h]
            km = rhs_k[h]
            uw = dot(jnp.concatenate([uh, ul, wh, wl], axis=1), jnp.concatenate([vm, vm, km, km], axis=0))
            uws.append(split(uw))
            uwbuf[h, 0:T, :] = uws[hh][0]
            uwbuf[h, T : 2 * T, :] = uws[hh][1]
        for hh in range(4):
            h = n * 4 + hh
            ktp = kt_ref[n * 2 + hh // 2, (hh % 2) * HD : (hh % 2) * HD + HD, :]
            bn = dot4(split(ktp * kds[hh]), uws[hh])
            if hh % 2:
                bn = roll64(bn)
            ident = jnp.where(lane64 - HD == sub64, tots[hh], 0.0)
            mb_out[h] = jnp.where(lane64 < HD, bn, ident - bn)
        for hh in range(4):
            h = n * 4 + hh

            @pl.when(h == sp)
            def _():
                mb_in[h] = mb_out[h]

            @pl.when(h != sp)
            def _():
                pltpu.make_async_remote_copy(
                    mb_out.at[h], mb_in.at[sp], mb_sem.at[0], mb_sem.at[1],
                    device_id=at(n, hh, y, c), device_id_type=MESH,
                ).start()

        return carry

    lax.fori_loop(0, 4, heads, 0)

    def inside(n, carry):
        col = cols.at[n]
        auws = []
        for hh in range(4):
            h = n * 4 + hh
            uw = uwbuf[h]
            auws.append(dot3(split(raw[h, T : 2 * T, :]), (uw[:T], uw[T:])))
        for jj in range(2):
            j = n * 2 + jj
            a, b = 2 * jj, 2 * jj + 1
            sc_a = col[:, a + 32 : a + 33] * jnp.exp(col[:, a : a + 1])
            sc_b = col[:, b + 32 : b + 33] * jnp.exp(col[:, b : b + 1])
            p = qroll[j] * jnp.where(low_half, sc_b, sc_a) - jnp.where(low_half, auws[b], auws[a])
            hi, lo = split(p)
            pbuf[j, :, 0:T] = hi
            pbuf[j, :, T : 2 * T] = lo
            oloc[j] = jnp.where(low_half, auws[a], auws[b])
        return carry

    lax.fori_loop(0, 4, inside, 0)

    many_recv(mb_in, 15, mb_sem.at[1])
    first = lane64 < HD
    eye = (lane64 & 63) == sub64
    ident_two = jnp.where(eye, 1.0, 0.0).astype(BF16)
    ident_one = jnp.where(eye & first, 1.0, 0.0).astype(BF16)
    zero = jnp.zeros((HD, T), BF16)

    def after(later, earlier, ident):
        hi, lo = split(earlier)
        return dot4(
            later, (jnp.concatenate([ident, hi], axis=0), jnp.concatenate([zero, lo], axis=0))
        )

    def added(step):
        return jnp.where(first, step, roll64(step))

    def keep(p, state):
        s_out[p] = jnp.where(first[: HD // 2], state[: HD // 2], state[HD // 2 :]).astype(BF16)

    steps = [mb_in[p] for p in range(15)]
    ones_ = [split(m) for m in steps]
    twos = [after(ones_[2 * i + 1], steps[2 * i], ident_one) for i in range(7)]
    twos_ = [split(m) for m in twos]
    fours = [after(twos_[2 * i + 1], twos[2 * i], ident_one) for i in range(3)]
    keep(0, jnp.zeros((HD, T), F32))
    state = added(fours[0])
    keep(1, added(steps[0]))
    two = added(twos[0])
    keep(2, two)
    keep(3, after(ones_[2], two, ident_two))
    keep(4, state)
    eight = after(split(fours[1]), state, ident_two)
    six = after(twos_[2], state, ident_two)
    keep(5, after(ones_[4], state, ident_two))
    keep(6, six)
    keep(7, after(ones_[6], six, ident_two))
    keep(8, eight)
    twelve = after(split(fours[2]), eight, ident_two)
    ten = after(twos_[4], eight, ident_two)
    keep(9, after(ones_[8], eight, ident_two))
    keep(10, ten)
    fourteen = after(twos_[6], twelve, ident_two)
    keep(11, after(ones_[10], ten, ident_two))
    keep(12, twelve)
    keep(13, after(ones_[12], twelve, ident_two))
    keep(14, fourteen)
    keep(15, after(ones_[14], fourteen, ident_two))

    def send_state(i, carry):
        p = (sp + i) & 15
        pltpu.make_async_remote_copy(
            s_out.at[p], s_in.at[sp], s_sem.at[0], s_sem.at[1],
            device_id=at(p >> 2, p, y, c), device_id_type=MESH,
        ).start()
        return carry

    lax.fori_loop(1, 16, send_state, 0)
    s_in[sp] = s_out[sp]

    many_recv(s_in, 15, s_sem.at[1])
    ones = jnp.where((iota((2 * T, T), 0) >> 6) & 1 == iota((2 * T, T), 1) >> 6, 1.0, 0.0).astype(BF16)
    for j in range(NH // 2):
        cut = slice(j * T, (j + 1) * T)
        even = s_in[2 * j].astype(F32)
        odd = s_in[2 * j + 1].astype(F32)
        head = first[: HD // 2]
        sj = jnp.concatenate(
            [
                jnp.where(head, 0.0, roll64(odd)), jnp.where(head, 0.0, odd),
                jnp.where(head, even, 0.0), jnp.where(head, roll64(even), 0.0),
            ],
            axis=0,
        ).astype(BF16)
        o = oloc[j] + dot(pbuf[j], jnp.concatenate([sj, sj], axis=0))
        hi, lo = split(o * o)
        mean = dot(jnp.concatenate([hi, lo], axis=1), ones) * (1.0 / HD)
        normed = (o * lax.rsqrt(mean + EPS) * hgain_ref[...]).astype(BF16)
        gated[:, cut] = (normed.astype(F32) * silu_g[:, cut]).astype(BF16)
    loads[4].wait()
    loads[5].wait()
    total = jnp.zeros((T, 1), F32)
    for n in range(4):
        cut = slice(n * 512, (n + 1) * 512)
        m = res_ref[:, cut].astype(F32) + dot(gated[...], om_ref[:, cut])
        mixed[:, cut] = m
        total = total + jnp.sum(m * m, axis=1, keepdims=True)
    inv = lax.rsqrt(total * (1.0 / D) + EPS)
    for h in range(2):
        cut = slice(h * HALF, (h + 1) * HALF)
        x2[h * T : (h + 1) * T, :] = (mixed[:, cut] * inv * egain_ref[:, cut]).astype(BF16)

    pl.semaphore_wait(all_in, 7)

    def dispatch(n, carry):
        block = dot(sel[pl.ds(n * 256, 256), :], x2[...]).astype(BF16)
        out_buf[pl.ds(n * PER, PER)] = block.reshape(PER, 8, HALF)

        def send(j, inner):
            i = n * PER + j
            dz, dx, dy, dc = offset(i)

            @pl.when(i != 0)
            def _():
                pltpu.make_async_remote_copy(
                    out_buf.at[i], arrived.at[i], fwd_send, fwd_recv.at[n],
                    device_id=at(z + dz, x + dx, y + dy, c + dc), device_id_type=MESH,
                ).start()

            return inner

        lax.fori_loop(0, PER, send, 0)
        return carry

    lax.fori_loop(0, CHUNKS, dispatch, 0)
    arrived[0] = out_buf[0]
    loads[6].wait()
    loads[7].wait()
    loads[8].wait()

    sub256 = iota((256, 256), 0)
    lane256 = iota((256, 256), 1)
    source = ((sub256 & 127) >> 2) * 8 + (sub256 >> 7) * 4 + (sub256 & 3)
    apart = jnp.where(source == lane256, 1.0, 0.0).astype(BF16)
    source = ((lane256 & 127) >> 2) * 8 + (lane256 >> 7) * 4 + (lane256 & 3)
    together = jnp.where(source == sub256, 1.0, 0.0).astype(BF16)

    def send_back(n):
        def send(j, inner):
            i = n * PER + j
            dz, dx, dy, dc = offset(i)

            @pl.when(i != 0)
            def _():
                pltpu.make_async_remote_copy(
                    prod.at[i], back.at[i], ret_send, ret_recv.at[n],
                    device_id=at(z - dz, x - dx, y - dy, c - dc), device_id_type=MESH,
                ).start()

            return inner

        lax.fori_loop(0, PER, send, 0)
    def expert(n, carry):
        @pl.when(n == 0)
        def _():
            many_recv(arrived, PER - 1, fwd_recv.at[0])

        @pl.when(n != 0)
        def _():
            many_recv(arrived, PER, fwd_recv.at[n])

        rows = arrived[pl.ds(n * PER, PER)].reshape(256, HALF)
        xs[...] = dot(apart, rows).astype(BF16)
        for k in range(4):
            cut = slice(k * 256, (k + 1) * 256)
            gate = dot(xs[0:T, :], wg_ref[0:HALF, cut]) + dot(xs[T : 2 * T, :], wg_ref[HALF:D, cut])
            upper = dot(xs[0:T, :], wu_ref[0:HALF, cut]) + dot(xs[T : 2 * T, :], wu_ref[HALF:D, cut])
            acc[:, cut] = (gate / (1.0 + jnp.exp(-gate)) * upper).astype(BF16)
        for k in range(8):
            cut = slice(k * 256, (k + 1) * 256)
            half, inside = k // 4, slice((k % 4) * 256, (k % 4 + 1) * 256)
            xs[half * T : (half + 1) * T, inside] = dot(acc[...], wd_ref[:, cut]).astype(BF16)
        prod[pl.ds(n * PER, PER)] = dot(together, xs[...]).astype(BF16).reshape(PER, 8, HALF)

        @pl.when(n >= 1)
        def _():
            send_back(n - 1)

        return carry

    lax.fori_loop(0, CHUNKS, expert, 0)
    send_back(3)
    back[0] = prod[0]

    for n in range(CHUNKS):
        many_recv(back, PER - 1 if n == 0 else PER, ret_recv.at[n])
        part = dot(wsel[:, n * 256 : (n + 1) * 256], back[n * PER : (n + 1) * PER].reshape(256, HALF))
        for h in range(2):
            cut = slice(h * HALF, (h + 1) * HALF)
            total = mixed[:, cut] + (part[h * T : (h + 1) * T] + part[(2 + h) * T : (3 + h) * T])
            if n < CHUNKS - 1:
                mixed[:, cut] = total
            else:
                out_ref[:, cut] = total.astype(BF16)

    many_sent(rates, 15, rate_sem.at[0])
    many_sent(mb_out, 15, mb_sem.at[0])
    many_sent(s_out, 15, s_sem.at[0])
    many_sent(out_buf, NE - 1, fwd_send)
    many_sent(prod, NE - 1, ret_send)


def call(*args):
    vm = pl.BlockSpec(memory_space=pltpu.VMEM)
    hbm = pl.BlockSpec(memory_space=pl.ANY)
    return pl.pallas_call(
        kernel,
        out_shape=pltpu.VMEM((T, D), BF16),
        in_specs=[vm] * 6 + [pl.BlockSpec(memory_space=pltpu.SMEM)] + [vm] * 2 + [hbm] * 9,
        out_specs=vm,
        scratch_shapes=[
            pltpu.VMEM((T, NH * HD), BF16),
            pltpu.VMEM((T, NH * HD), BF16),
            pltpu.VMEM((T, NH * HD), BF16),
            pltpu.VMEM((T, NH * HD), BF16),
            pltpu.VMEM((T, D), BF16),
            pltpu.VMEM((NH * HD, D), BF16),
            pltpu.VMEM((D, FF), BF16),
            pltpu.VMEM((D, FF), BF16),
            pltpu.VMEM((FF, D), BF16),
            pltpu.VMEM((T, T), F32),
            pltpu.VMEM((8, T), F32),
            pltpu.VMEM((1, T), F32),
            pltpu.VMEM((16, 8, T), F32),
            pltpu.VMEM((NH, 2 * T, T), F32),
            pltpu.VMEM((NH // 2, T, T), F32),
            pltpu.VMEM((NH, T, T), BF16),
            pltpu.VMEM((NH, T, T), BF16),
            pltpu.VMEM((NH // 2, T, T), F32),
            pltpu.VMEM((T, NH * HD), F32),
            pltpu.VMEM((4, T, T), F32),
            pltpu.VMEM((T, T), F32),
            pltpu.VMEM((NH, 2 * T, T), BF16),
            pltpu.VMEM((NH, HD, T), F32),
            pltpu.VMEM((NH, HD, T), F32),
            pltpu.VMEM((NH, HD // 2, T), BF16),
            pltpu.VMEM((NH, HD // 2, T), BF16),
            pltpu.VMEM((NH // 2, T, T), F32),
            pltpu.VMEM((NH // 2, T, 2 * T), BF16),
            pltpu.VMEM((T, NH * HD), BF16),
            pltpu.VMEM((T, D), F32),
            pltpu.VMEM((2 * T, HALF), BF16),
            pltpu.VMEM((NE * 8, 2 * T), BF16),
            pltpu.VMEM((4 * T, NE * 8), BF16),
            pltpu.VMEM((NE, 8, HALF), BF16),
            pltpu.VMEM((NE, 8, HALF), BF16),
            pltpu.VMEM((NE, 8, HALF), BF16),
            pltpu.VMEM((NE, 8, HALF), BF16),
            pltpu.VMEM((2 * T, HALF), BF16),
            pltpu.VMEM((T, FF), BF16),
            pltpu.SemaphoreType.DMA((9,)),
            pltpu.SemaphoreType.DMA((2,)),
            pltpu.SemaphoreType.DMA((2,)),
            pltpu.SemaphoreType.DMA((2,)),
            pltpu.SemaphoreType.DMA,
            pltpu.SemaphoreType.DMA((CHUNKS,)),
            pltpu.SemaphoreType.DMA,
            pltpu.SemaphoreType.DMA((CHUNKS,)),
            pltpu.SemaphoreType.REGULAR,
        ],
        compiler_params=pltpu.CompilerParams(
            collective_id=0, has_side_effects=True, vmem_limit_bytes=60 * 1024 * 1024
        ),
        name="layer",
    )(*args)


def shards(
    residual, query, key, value, output_gate, write_logits, decay_logits, extra_decay, head_rate,
    head_gain, output_matrix, expert_gain, group_scores, expert_scores, routes,
    gate_weight, up_weight, down_weight,
):
    out = call(
        write_logits[0].T, decay_logits[0].T, extra_decay[0].T, group_scores[0].T, expert_scores[0].T,
        routes[0].T, head_rate, head_gain[None], expert_gain[None], query[0], key[0], value[0],
        output_gate[0], residual[0], output_matrix, gate_weight[0], up_weight[0], down_weight[0],
    )
    return out[None]


def solution(mesh):
    tok = P("dp", "sp", None)
    exp = P(("sp", "dp"), None, None)
    in_specs = (
        (tok,) * 8 + (P("sp"), P(), P(), P()) + (tok,) * 3 + (exp,) * 3
    )
    return jax.shard_map(shards, mesh=mesh, in_specs=in_specs, out_specs=tok, check_vma=False)
```

```python
import jax
import jax.numpy as jnp
from jax import lax
from jax.experimental import pallas as pl
from jax.experimental.pallas import tpu as pltpu
from jax.sharding import PartitionSpec as P

F32 = jnp.float32
BF16 = jnp.bfloat16
MESH = pl.DeviceIdType.MESH
EPS = 1e-06
T = 128
HD = 64
NH = 16
D = 2048
HALF = D // 2
FF = 1024
NE = 128
CHUNKS = 4
PER = NE // CHUNKS
OWN = 122


def coords():
    sp = lax.axis_index("sp")
    dp = lax.axis_index("dp")
    return sp >> 2, sp & 3, dp >> 1, dp & 1


def at(z, x, y, c):
    return (((z & 3) << 2) + (x & 3), ((y & 3) << 1) + (c & 1))


def offset(i):
    chunk = 3 - (i >> 5)
    dx = (i & 3) ^ 2
    dy = ((i >> 2) & 3) ^ 2
    return (chunk - dx - dy) & 3, dx, dy, 1 - ((i >> 4) & 1)


def iota(shape, dim):
    return lax.broadcasted_iota(jnp.int32, shape, dim)


def split(a):
    hi = a.astype(BF16)
    return hi, (a - hi.astype(F32)).astype(BF16)


def dot(a, b):
    return jnp.dot(a, b, preferred_element_type=F32)


def dot3(a, b):
    (ah, al), (bh, bl) = a, b
    return dot(jnp.concatenate([ah, ah, al], axis=1), jnp.concatenate([bh, bl, bh], axis=0))


def dot4(a, b):
    (ah, al), (bh, bl) = a, b
    left = jnp.concatenate(
        [jnp.concatenate([ah, ah], axis=1), jnp.concatenate([al, al], axis=1)], axis=0
    )
    both = dot(left, jnp.concatenate([bh, bl], axis=0))
    return both[: ah.shape[0]] + both[ah.shape[0] :]


def odd_blocks(a, size):
    return jnp.concatenate([a[i : i + size] for i in range(size, T, 2 * size)], axis=0)


def with_odd_blocks(even, odd, size):
    parts = []
    for n, i in enumerate(range(0, T, 2 * size)):
        parts += [even[i : i + size], odd[n * size : (n + 1) * size]]
    return jnp.concatenate(parts, axis=0)


def roll64(a):
    return pltpu.roll(a, 64, 1)


def kernel(
    wsl_ref, dl_ref, el_ref, grs_ref, ces_ref, routes_ref, rate_in, hg_ref, egain_ref,
    q_hbm, k_hbm, v_hbm, gate_hbm, res_hbm, om_hbm, wg_hbm, wu_hbm, wd_hbm,
    out_ref,
    q_ref, k_ref, v_ref, gate_ref, res_ref, om_ref, wg_ref, wu_ref, wd_ref,
    small_rows, rate_ref, hgain_ref, rates, raw, kt_ref, rhs_v, rhs_k, qroll, silu_g, cols, rows_ref,
    uwbuf, mb_out, mb_in, s_out, s_in, oloc, pbuf, gated, mixed, x2,
    sel, wsel, out_buf, arrived, prod, back, xs, acc,
    load_sem, rate_sem, mb_sem, s_sem, fwd_send, fwd_recv, ret_send, ret_recv, all_in,
):
    z, x, y, c = coords()
    sp = (z << 2) + x
    partner = at(z, x, y, c + 1)

    loads = [
        pltpu.make_async_copy(src, dst, load_sem.at[i])
        for i, (src, dst) in enumerate(
            (
                (k_hbm, k_ref), (q_hbm, q_ref), (v_hbm, v_ref), (gate_hbm, gate_ref),
                (res_hbm, res_ref), (om_hbm, om_ref),
                (wg_hbm, wg_ref), (wu_hbm, wu_ref), (wd_hbm, wd_ref),
            )
        )
    ]
    for copy in loads:
        copy.start()

    barrier = pltpu.get_barrier_semaphore()

    def greet_sp(i, carry):
        pl.semaphore_signal(barrier, 1, device_id=at(z + (i >> 2), x + i, y, c), device_id_type=MESH)
        return carry

    def greet_dp(i, carry):
        pl.semaphore_signal(barrier, 1, device_id=at(z, x, y + (i >> 1), c + i), device_id_type=MESH)
        return carry

    lax.fori_loop(1, 16, greet_sp, 0)
    lax.fori_loop(1, 8, greet_dp, 0)

    def many_recv(buf, count, sem):
        part = buf.at[pl.ds(0, count)]
        pltpu.make_async_remote_copy(part, part, sem, sem, device_id=partner, device_id_type=MESH).wait_recv()

    def many_sent(buf, count, sem):
        part = buf.at[pl.ds(0, count)]
        pltpu.make_async_remote_copy(part, part, sem, sem, device_id=partner, device_id_type=MESH).wait_send()

    lane = iota((T, T), 1)
    sub = iota((T, T), 0)
    low_half = lane < HD

    rate_ref[...] = jnp.full((8, T), rate_in[0], F32)
    hgain_ref[:, 0:HD] = hg_ref[...]
    hgain_ref[:, HD:T] = hg_ref[...]
    small_rows[...] = jnp.zeros((T, T), F32)
    small_rows[0:16, :] = wsl_ref[...]
    small_rows[16:32, :] = dl_ref[...]
    small_rows[32:48, :] = el_ref[...]
    small_rows[48:52, :] = grs_ref[...]
    small_rows[52:54, :] = ces_ref[...]
    small_rows[54:56, :] = routes_ref[...].astype(F32)
    small = jnp.transpose(small_rows[...])
    e0 = small[:, 54:55].astype(jnp.int32)
    e1 = small[:, 55:56].astype(jnp.int32)
    one0 = jnp.where(lane == e0, 1.0, 0.0)
    one1 = jnp.where(lane == e1, 1.0, 0.0)
    before = dot(jnp.where(sub > lane, 1.0, 0.0).astype(BF16), (one0 + one1).astype(BF16))
    rank0 = jnp.sum(before * one0, axis=1, keepdims=True).astype(jnp.int32)
    rank1 = jnp.sum(before * one1, axis=1, keepdims=True).astype(jnp.int32)

    def slot_of(e, rank):
        dz = ((e >> 5) - z) & 3
        dx = ((e >> 3) - x) & 3
        dy = ((e >> 1) - y) & 3
        dc = (e - c) & 1
        chunk = 3 - ((dz + dx + dy) & 3)
        return ((chunk << 5) + ((1 - dc) << 4) + ((dy ^ 2) << 2) + (dx ^ 2)) * 8 + rank

    slot0 = slot_of(e0, rank0)
    slot1 = slot_of(e1, rank1)
    scores = jnp.exp(small)
    is_group = (lane >= 48) & (lane < 52)
    is_pick = (lane >= 52) & (lane < 54)
    own_group = lane == (e0 >> 5) + 48
    group_sum = jnp.sum(jnp.where(is_group, scores, 0.0), axis=1, keepdims=True)
    group_own = jnp.sum(jnp.where(own_group, scores, 0.0), axis=1, keepdims=True)
    pick_sum = jnp.sum(jnp.where(is_pick, scores, 0.0), axis=1, keepdims=True)
    prob = group_own / group_sum
    w0 = prob * scores[:, 52:53] / pick_sum
    w1 = prob * scores[:, 53:54] / pick_sum
    wide = iota((T, NE * 8), 1)
    for h in range(2):
        w = jnp.where(wide == slot0 + 4 * h, w0, 0.0) + jnp.where(wide == slot1 + 4 * h, w1, 0.0)
        hi, lo = split(w)
        wsel[h * T : (h + 1) * T, :] = hi
        wsel[(2 + h) * T : (3 + h) * T, :] = lo
    slot_cols = jnp.where(lane == 0, slot0.astype(F32), slot1.astype(F32))
    slot_rows = jnp.transpose(slot_cols)
    row0 = slot_rows[0:1, :].astype(jnp.int32)
    row1 = slot_rows[1:2, :].astype(jnp.int32)
    tall = iota((NE * 8, T), 0)
    for h in range(2):
        hit = (tall == row0 + 4 * h) | (tall == row1 + 4 * h)
        sel[:, h * T : (h + 1) * T] = jnp.where(hit, 1.0, 0.0).astype(BF16)

    loads[0].wait()
    loads[1].wait()
    loads[2].wait()
    sums = jnp.zeros((2 * T, T), F32)
    sel_row = iota((2 * T, T), 0)
    sel_lane = iota((2 * T, T), 1)
    sel_head = (sel_row & 127) >> 6
    for j in range(NH // 2):
        cut = slice(j * T, (j + 1) * T)
        kb = k_ref[:, cut]
        qb = q_ref[:, cut]
        k32 = kb.astype(F32)
        q32 = qb.astype(F32)
        hi, lo = split(jnp.concatenate([k32 * k32, q32 * q32], axis=0))
        pick = jnp.where(sel_lane == sel_head + 2 * j, 1.0, 0.0).astype(BF16)
        sums = sums + dot(jnp.concatenate([hi, lo], axis=1), pick)
        kt = jnp.transpose(k32)
        kt_ref[j] = kt
        both = jnp.concatenate(
            [jnp.where(sub < HD, kt, 0.0), jnp.where(sub < HD, 0.0, kt)], axis=1
        ).astype(BF16)
        prods = dot(jnp.concatenate([kb, qb], axis=0), both)
        raw[2 * j] = prods[:, :T]
        raw[2 * j + 1] = prods[:, T:]
        v32 = v_ref[:, cut].astype(F32)
        kr = roll64(k32)
        rhs_v[2 * j] = jnp.where(low_half, v32, 0.0).astype(BF16)
        rhs_v[2 * j + 1] = jnp.where(low_half, 0.0, v32).astype(BF16)
        rhs_k[2 * j] = jnp.where(low_half, 0.0, kr).astype(BF16)
        rhs_k[2 * j + 1] = jnp.where(low_half, kr, 0.0).astype(BF16)
        qroll[j] = roll64(q32)
    inv = lax.rsqrt(sums + EPS)
    rk = inv[:T]
    rq = inv[T:] * (HD**-0.5)
    loads[3].wait()
    for j in range(NH // 2):
        cut = slice(j * T, (j + 1) * T)
        v32 = gate_ref[:, cut].astype(F32)
        silu_g[:, cut] = v32 / (1.0 + jnp.exp(-v32))

    pl.semaphore_wait(barrier, 22)

    def send_rate(i, carry):
        pltpu.make_async_remote_copy(
            rate_ref, rates.at[sp], rate_sem.at[0], rate_sem.at[1],
            device_id=at(z + (i >> 2), x + i, y, c), device_id_type=MESH,
        ).start()
        return carry

    lax.fori_loop(1, 16, send_rate, 0)

    def tell_in(i, carry):
        pl.semaphore_signal(all_in, 1, device_id=at(z, x, y + (i >> 1), c + i), device_id_type=MESH)
        return carry

    lax.fori_loop(1, 8, tell_in, 0)
    rates[sp] = rate_ref[...]
    is_head = lane < NH
    beta = jax.nn.sigmoid(jnp.where(is_head, small, 0.0))
    dl = jnp.where(is_head, pltpu.roll(small, T - 16, 1), 0.0)
    el = jnp.where(is_head, pltpu.roll(small, T - 32, 1), 0.0)
    soft = jax.nn.softplus(dl)
    many_recv(rates, 15, rate_sem.at[1])
    eye16 = iota((NH, T), 0) == iota((NH, T), 1)
    rate_row = jnp.sum(jnp.where(eye16, rates[:, 0, :], 0.0), axis=0, keepdims=True)
    g = jnp.where(is_head, el - rate_row * soft, 0.0)
    g1 = g.astype(BF16)
    rest = g - g1.astype(F32)
    g2, g3 = split(rest)
    tri = jnp.where(sub >= lane, 1.0, 0.0).astype(BF16)
    cumul = dot(jnp.concatenate([tri, tri, tri], axis=1), jnp.concatenate([g1, g2, g3], axis=0))
    packed = (
        jnp.where(is_head, cumul, 0.0)
        + pltpu.roll(jnp.where(is_head, rk, 0.0), 16, 1)
        + pltpu.roll(jnp.where(is_head, beta, 0.0), 32, 1)
        + pltpu.roll(jnp.where(is_head, rq, 0.0), 48, 1)
    )
    rows_ref[...] = jnp.transpose(packed)
    colpack = (
        jnp.where(is_head, cumul, 0.0)
        + pltpu.roll(jnp.where(is_head, beta * rk, 0.0), 16, 1)
        + pltpu.roll(jnp.where(is_head, rq, 0.0), 32, 1)
    )
    cols[0] = colpack
    for n in range(1, 4):
        cols[n] = pltpu.roll(colpack, T - 4 * n, 1)

    lane64 = iota((HD, T), 1)
    sub64 = iota((HD, T), 0)

    def heads(step, carry):
        base = 8 * (((z >> 1) + 1 - step) & 1)
        causal = sub >= lane
        ls, ups, ws, kds, tots = [], [], [], [], []
        for hh in range(8):
            h = base + hh
            col = cols.at[h >> 2]
            cc = hh % 4
            c_row = rows_ref[pl.ds(h, 1), :]
            k_row = rows_ref[pl.ds(h + 16, 1), :]
            b_row = rows_ref[pl.ds(h + 32, 1), :]
            c_col = col[:, cc : cc + 1]
            dec = jnp.where(causal, jnp.exp(jnp.minimum(c_col - c_row, 0.0)), 0.0) * k_row
            ls.append(jnp.where(sub > lane, raw[h, 0:T, :] * dec * col[:, cc + 16 : cc + 17], 0.0))
            raw[h, T : 2 * T, :] = raw[h, T : 2 * T, :] * dec * col[:, cc + 32 : cc + 33]
            ups.append(b_row)
            ws.append(b_row * k_row * jnp.exp(c_row))
            last = c_row[:, T - 1 : T]
            kds.append(k_row * jnp.exp(last - c_row))
            tots.append(jnp.exp(last))
        ts = []
        pairs = (sub >> 1) == (lane >> 1)
        m = ((sub >> 1) == (lane >> 1) + 1) & (((sub >> 1) & 1) == 1)
        for l in ls:
            near = jnp.where(pairs, l, 0.0)
            far = jnp.where(m, l, 0.0)
            far = far - pltpu.roll(far, T - 1, 1) * jnp.sum(near, axis=0, keepdims=True)
            far = far - pltpu.roll(far, 1, 0) * jnp.sum(near, axis=1, keepdims=True)
            ts.append(jnp.where(sub == lane, 1.0, 0.0) - near - far)
        m = ((sub >> 2) == (lane >> 2) + 1) & (((sub >> 2) & 1) == 1)
        tsp = [split(t) for t in ts]
        xsp = [split(dot3(split(jnp.where(m, l, 0.0)), t)) for l, t in zip(ls, tsp)]
        ts = [t - dot3(tp, xx) for t, tp, xx in zip(ts, tsp, xsp)]
        for bits in range(3, 7):
            size = 1 << bits
            m = (lane64 >> bits) == 2 * (sub64 >> bits)
            none = jnp.zeros((T, T), F32)
            xs_ = [dot4(split(jnp.where(m, odd_blocks(l, size), 0.0)), split(t)) for l, t in zip(ls, ts)]
            odd = [odd_blocks(t, size) for t in ts]
            ys_ = [dot4(split(o), split(with_odd_blocks(none, x_, size))) for o, x_ in zip(odd, xs_)]
            ts = [with_odd_blocks(t, o - y_, size) for t, o, y_ in zip(ts, odd, ys_)]
        uws = []
        for hh in range(8):
            h = base + hh
            uh, ul = split(ts[hh] * ups[hh])
            wh, wl = split(ts[hh] * ws[hh])
            vm = rhs_v[h]
            km = rhs_k[h]
            uw = dot(jnp.concatenate([uh, ul, wh, wl], axis=1), jnp.concatenate([vm, vm, km, km], axis=0))
            uws.append(split(uw))
            uwbuf[h, 0:T, :] = uws[hh][0]
            uwbuf[h, T : 2 * T, :] = uws[hh][1]
        for hh in range(8):
            h = base + hh
            ktp = kt_ref[h >> 1, (hh % 2) * HD : (hh % 2) * HD + HD, :]
            bn = dot4(split(ktp * kds[hh]), uws[hh])
            if hh % 2:
                bn = roll64(bn)
            ident = jnp.where(lane64 - HD == sub64, tots[hh], 0.0)
            mb_out[h] = jnp.where(lane64 < HD, bn, ident - bn)
        for hh in range(8):
            h = base + hh

            @pl.when(h == sp)
            def _():
                mb_in[h] = mb_out[h]

            @pl.when(h != sp)
            def _():
                pltpu.make_async_remote_copy(
                    mb_out.at[h], mb_in.at[sp], mb_sem.at[0], mb_sem.at[1],
                    device_id=at(h >> 2, hh, y, c), device_id_type=MESH,
                ).start()

        return carry

    lax.fori_loop(0, 2, heads, 0)

    def inside(n, carry):
        col = cols.at[n]
        auws = []
        for hh in range(4):
            h = n * 4 + hh
            uw = uwbuf[h]
            auws.append(dot3(split(raw[h, T : 2 * T, :]), (uw[:T], uw[T:])))
        for jj in range(2):
            j = n * 2 + jj
            a, b = 2 * jj, 2 * jj + 1
            sc_a = col[:, a + 32 : a + 33] * jnp.exp(col[:, a : a + 1])
            sc_b = col[:, b + 32 : b + 33] * jnp.exp(col[:, b : b + 1])
            p = qroll[j] * jnp.where(low_half, sc_b, sc_a) - jnp.where(low_half, auws[b], auws[a])
            hi, lo = split(p)
            pbuf[j, :, 0:T] = hi
            pbuf[j, :, T : 2 * T] = lo
            oloc[j] = jnp.where(low_half, auws[a], auws[b])
        return carry

    lax.fori_loop(0, 4, inside, 0)

    many_recv(mb_in, 15, mb_sem.at[1])
    first = lane64 < HD
    eye = (lane64 & 63) == sub64
    ident_two = jnp.where(eye, 1.0, 0.0).astype(BF16)
    ident_one = jnp.where(eye & first, 1.0, 0.0).astype(BF16)
    zero = jnp.zeros((HD, T), BF16)

    def after(later, earlier, ident):
        hi, lo = split(earlier)
        return dot4(
            later, (jnp.concatenate([ident, hi], axis=0), jnp.concatenate([zero, lo], axis=0))
        )

    def added(step):
        return jnp.where(first, step, roll64(step))

    def keep(p, state):
        s_out[p] = jnp.where(first[: HD // 2], state[: HD // 2], state[HD // 2 :]).astype(BF16)

    steps = [mb_in[p] for p in range(15)]
    ones_ = [split(m) for m in steps]
    twos = [after(ones_[2 * i + 1], steps[2 * i], ident_one) for i in range(7)]
    twos_ = [split(m) for m in twos]
    fours = [after(twos_[2 * i + 1], twos[2 * i], ident_one) for i in range(3)]
    keep(0, jnp.zeros((HD, T), F32))
    state = added(fours[0])
    keep(1, added(steps[0]))
    two = added(twos[0])
    keep(2, two)
    keep(3, after(ones_[2], two, ident_two))
    keep(4, state)
    eight = after(split(fours[1]), state, ident_two)
    six = after(twos_[2], state, ident_two)
    keep(5, after(ones_[4], state, ident_two))
    keep(6, six)
    keep(7, after(ones_[6], six, ident_two))
    keep(8, eight)
    twelve = after(split(fours[2]), eight, ident_two)
    ten = after(twos_[4], eight, ident_two)
    keep(9, after(ones_[8], eight, ident_two))
    keep(10, ten)
    fourteen = after(twos_[6], twelve, ident_two)
    keep(11, after(ones_[10], ten, ident_two))
    keep(12, twelve)
    keep(13, after(ones_[12], twelve, ident_two))
    keep(14, fourteen)
    keep(15, after(ones_[14], fourteen, ident_two))

    def send_state(i, carry):
        p = (sp + i) & 15
        pltpu.make_async_remote_copy(
            s_out.at[p], s_in.at[sp], s_sem.at[0], s_sem.at[1],
            device_id=at(p >> 2, p, y, c), device_id_type=MESH,
        ).start()
        return carry

    lax.fori_loop(1, 16, send_state, 0)
    s_in[sp] = s_out[sp]

    many_recv(s_in, 15, s_sem.at[1])
    ones = jnp.where((iota((2 * T, T), 0) >> 6) & 1 == iota((2 * T, T), 1) >> 6, 1.0, 0.0).astype(BF16)
    for j in range(NH // 2):
        cut = slice(j * T, (j + 1) * T)
        even = s_in[2 * j].astype(F32)
        odd = s_in[2 * j + 1].astype(F32)
        head = first[: HD // 2]
        sj = jnp.concatenate(
            [
                jnp.where(head, 0.0, roll64(odd)), jnp.where(head, 0.0, odd),
                jnp.where(head, even, 0.0), jnp.where(head, roll64(even), 0.0),
            ],
            axis=0,
        ).astype(BF16)
        o = oloc[j] + dot(pbuf[j], jnp.concatenate([sj, sj], axis=0))
        hi, lo = split(o * o)
        mean = dot(jnp.concatenate([hi, lo], axis=1), ones) * (1.0 / HD)
        normed = (o * lax.rsqrt(mean + EPS) * hgain_ref[...]).astype(BF16)
        gated[:, cut] = (normed.astype(F32) * silu_g[:, cut]).astype(BF16)
    loads[4].wait()
    loads[5].wait()
    total = jnp.zeros((T, 1), F32)
    for n in range(4):
        cut = slice(n * 512, (n + 1) * 512)
        m = res_ref[:, cut].astype(F32) + dot(gated[...], om_ref[:, cut])
        mixed[:, cut] = m
        total = total + jnp.sum(m * m, axis=1, keepdims=True)
    inv = lax.rsqrt(total * (1.0 / D) + EPS)
    for h in range(2):
        cut = slice(h * HALF, (h + 1) * HALF)
        x2[h * T : (h + 1) * T, :] = (mixed[:, cut] * inv * egain_ref[:, cut]).astype(BF16)

    pl.semaphore_wait(all_in, 7)

    def dispatch(n, carry):
        block = dot(sel[pl.ds(n * 256, 256), :], x2[...]).astype(BF16)
        out_buf[pl.ds(n * PER, PER)] = block.reshape(PER, 8, HALF)

        def send(j, inner):
            i = n * PER + j
            dz, dx, dy, dc = offset(i)

            @pl.when(i != OWN)
            def _():
                pltpu.make_async_remote_copy(
                    out_buf.at[i], arrived.at[i], fwd_send, fwd_recv.at[n],
                    device_id=at(z + dz, x + dx, y + dy, c + dc), device_id_type=MESH,
                ).start()

            return inner

        lax.fori_loop(0, PER, send, 0)
        return carry

    lax.fori_loop(0, CHUNKS, dispatch, 0)
    arrived[OWN] = out_buf[OWN]
    loads[6].wait()
    loads[7].wait()
    loads[8].wait()

    sub256 = iota((256, 256), 0)
    lane256 = iota((256, 256), 1)
    source = ((sub256 & 127) >> 2) * 8 + (sub256 >> 7) * 4 + (sub256 & 3)
    apart = jnp.where(source == lane256, 1.0, 0.0).astype(BF16)
    source = ((lane256 & 127) >> 2) * 8 + (lane256 >> 7) * 4 + (lane256 & 3)
    together = jnp.where(source == sub256, 1.0, 0.0).astype(BF16)

    def send_back(n):
        def send(j, inner):
            i = n * PER + j
            dz, dx, dy, dc = offset(i)

            @pl.when(i != OWN)
            def _():
                pltpu.make_async_remote_copy(
                    prod.at[i], back.at[i], ret_send, ret_recv.at[n],
                    device_id=at(z - dz, x - dx, y - dy, c - dc), device_id_type=MESH,
                ).start()

            return inner

        lax.fori_loop(0, PER, send, 0)
    def expert(n, carry):
        @pl.when(n == 3)
        def _():
            many_recv(arrived, PER - 1, fwd_recv.at[3])

        @pl.when(n != 3)
        def _():
            many_recv(arrived, PER, fwd_recv.at[n])

        @pl.when(n >= 1)
        def _():
            send_back(n - 1)

        rows = arrived[pl.ds(n * PER, PER)].reshape(256, HALF)
        xs[...] = dot(apart, rows).astype(BF16)
        for k in range(4):
            cut = slice(k * 256, (k + 1) * 256)
            gate = dot(xs[0:T, :], wg_ref[0:HALF, cut]) + dot(xs[T : 2 * T, :], wg_ref[HALF:D, cut])
            upper = dot(xs[0:T, :], wu_ref[0:HALF, cut]) + dot(xs[T : 2 * T, :], wu_ref[HALF:D, cut])
            acc[:, cut] = (gate / (1.0 + jnp.exp(-gate)) * upper).astype(BF16)
        for k in range(8):
            cut = slice(k * 256, (k + 1) * 256)
            half, inside = k // 4, slice((k % 4) * 256, (k % 4 + 1) * 256)
            xs[half * T : (half + 1) * T, inside] = dot(acc[...], wd_ref[:, cut]).astype(BF16)
        prod[pl.ds(n * PER, PER)] = dot(together, xs[...]).astype(BF16).reshape(PER, 8, HALF)

        return carry

    lax.fori_loop(0, CHUNKS, expert, 0)
    send_back(3)
    back[OWN] = prod[OWN]

    for n in range(CHUNKS):
        many_recv(back, PER - 1 if n == 3 else PER, ret_recv.at[n])
        part = dot(wsel[:, n * 256 : (n + 1) * 256], back[n * PER : (n + 1) * PER].reshape(256, HALF))
        for h in range(2):
            cut = slice(h * HALF, (h + 1) * HALF)
            total = mixed[:, cut] + (part[h * T : (h + 1) * T] + part[(2 + h) * T : (3 + h) * T])
            if n < CHUNKS - 1:
                mixed[:, cut] = total
            else:
                out_ref[:, cut] = total.astype(BF16)

    many_sent(rates, 15, rate_sem.at[0])
    many_sent(mb_out, 15, mb_sem.at[0])
    many_sent(s_out, 15, s_sem.at[0])
    many_sent(out_buf, NE - 1, fwd_send)
    many_sent(prod, NE - 1, ret_send)


def call(*args):
    vm = pl.BlockSpec(memory_space=pltpu.VMEM)
    hbm = pl.BlockSpec(memory_space=pl.ANY)
    return pl.pallas_call(
        kernel,
        out_shape=pltpu.VMEM((T, D), BF16),
        in_specs=[vm] * 6 + [pl.BlockSpec(memory_space=pltpu.SMEM)] + [vm] * 2 + [hbm] * 9,
        out_specs=vm,
        scratch_shapes=[
            pltpu.VMEM((T, NH * HD), BF16),
            pltpu.VMEM((T, NH * HD), BF16),
            pltpu.VMEM((T, NH * HD), BF16),
            pltpu.VMEM((T, NH * HD), BF16),
            pltpu.VMEM((T, D), BF16),
            pltpu.VMEM((NH * HD, D), BF16),
            pltpu.VMEM((D, FF), BF16),
            pltpu.VMEM((D, FF), BF16),
            pltpu.VMEM((FF, D), BF16),
            pltpu.VMEM((T, T), F32),
            pltpu.VMEM((8, T), F32),
            pltpu.VMEM((1, T), F32),
            pltpu.VMEM((16, 8, T), F32),
            pltpu.VMEM((NH, 2 * T, T), F32),
            pltpu.VMEM((NH // 2, T, T), F32),
            pltpu.VMEM((NH, T, T), BF16),
            pltpu.VMEM((NH, T, T), BF16),
            pltpu.VMEM((NH // 2, T, T), F32),
            pltpu.VMEM((T, NH * HD), F32),
            pltpu.VMEM((4, T, T), F32),
            pltpu.VMEM((T, T), F32),
            pltpu.VMEM((NH, 2 * T, T), BF16),
            pltpu.VMEM((NH, HD, T), F32),
            pltpu.VMEM((NH, HD, T), F32),
            pltpu.VMEM((NH, HD // 2, T), BF16),
            pltpu.VMEM((NH, HD // 2, T), BF16),
            pltpu.VMEM((NH // 2, T, T), F32),
            pltpu.VMEM((NH // 2, T, 2 * T), BF16),
            pltpu.VMEM((T, NH * HD), BF16),
            pltpu.VMEM((T, D), F32),
            pltpu.VMEM((2 * T, HALF), BF16),
            pltpu.VMEM((NE * 8, 2 * T), BF16),
            pltpu.VMEM((4 * T, NE * 8), BF16),
            pltpu.VMEM((NE, 8, HALF), BF16),
            pltpu.VMEM((NE, 8, HALF), BF16),
            pltpu.VMEM((NE, 8, HALF), BF16),
            pltpu.VMEM((NE, 8, HALF), BF16),
            pltpu.VMEM((2 * T, HALF), BF16),
            pltpu.VMEM((T, FF), BF16),
            pltpu.SemaphoreType.DMA((9,)),
            pltpu.SemaphoreType.DMA((2,)),
            pltpu.SemaphoreType.DMA((2,)),
            pltpu.SemaphoreType.DMA((2,)),
            pltpu.SemaphoreType.DMA,
            pltpu.SemaphoreType.DMA((CHUNKS,)),
            pltpu.SemaphoreType.DMA,
            pltpu.SemaphoreType.DMA((CHUNKS,)),
            pltpu.SemaphoreType.REGULAR,
        ],
        compiler_params=pltpu.CompilerParams(
            collective_id=0, has_side_effects=True, vmem_limit_bytes=60 * 1024 * 1024
        ),
        name="layer",
    )(*args)


def shards(
    residual, query, key, value, output_gate, write_logits, decay_logits, extra_decay, head_rate,
    head_gain, output_matrix, expert_gain, group_scores, expert_scores, routes,
    gate_weight, up_weight, down_weight,
):
    out = call(
        write_logits[0].T, decay_logits[0].T, extra_decay[0].T, group_scores[0].T, expert_scores[0].T,
        routes[0].T, head_rate, head_gain[None], expert_gain[None], query[0], key[0], value[0],
        output_gate[0], residual[0], output_matrix, gate_weight[0], up_weight[0], down_weight[0],
    )
    return out[None]


def solution(mesh):
    tok = P("dp", "sp", None)
    exp = P(("sp", "dp"), None, None)
    in_specs = (
        (tok,) * 8 + (P("sp"), P(), P(), P()) + (tok,) * 3 + (exp,) * 3
    )
    return jax.shard_map(shards, mesh=mesh, in_specs=in_specs, out_specs=tok, check_vma=False)
```

```python
import jax
import jax.numpy as jnp
from jax import lax
from jax.experimental import pallas as pl
from jax.experimental.pallas import tpu as pltpu
from jax.sharding import PartitionSpec as P

F32 = jnp.float32
BF16 = jnp.bfloat16
MESH = pl.DeviceIdType.MESH
EPS = 1e-06
T = 128
HD = 64
NH = 16
D = 2048
HALF = D // 2
FF = 1024
NE = 128
CHUNKS = 4
PER = NE // CHUNKS
FAR = (10, 2, 8, 6, 14, 9, 11, 1, 3, 4, 12, 5, 7, 13, 15)
OWN = 122


def coords():
    sp = lax.axis_index("sp")
    dp = lax.axis_index("dp")
    return sp >> 2, sp & 3, dp >> 1, dp & 1


def at(z, x, y, c):
    return (((z & 3) << 2) + (x & 3), ((y & 3) << 1) + (c & 1))


def offset(i):
    chunk = 3 - (i >> 5)
    dx = (i & 3) ^ 2
    dy = ((i >> 2) & 3) ^ 2
    return (chunk - dx - dy) & 3, dx, dy, 1 - ((i >> 4) & 1)


def iota(shape, dim):
    return lax.broadcasted_iota(jnp.int32, shape, dim)


def split(a):
    hi = a.astype(BF16)
    return hi, (a - hi.astype(F32)).astype(BF16)


def dot(a, b):
    return jnp.dot(a, b, preferred_element_type=F32)


def dot3(a, b):
    (ah, al), (bh, bl) = a, b
    return dot(jnp.concatenate([ah, ah, al], axis=1), jnp.concatenate([bh, bl, bh], axis=0))


def dot4(a, b):
    (ah, al), (bh, bl) = a, b
    left = jnp.concatenate(
        [jnp.concatenate([ah, ah], axis=1), jnp.concatenate([al, al], axis=1)], axis=0
    )
    both = dot(left, jnp.concatenate([bh, bl], axis=0))
    return both[: ah.shape[0]] + both[ah.shape[0] :]


def odd_blocks(a, size):
    return jnp.concatenate([a[i : i + size] for i in range(size, T, 2 * size)], axis=0)


def with_odd_blocks(even, odd, size):
    parts = []
    for n, i in enumerate(range(0, T, 2 * size)):
        parts += [even[i : i + size], odd[n * size : (n + 1) * size]]
    return jnp.concatenate(parts, axis=0)


def roll64(a):
    return pltpu.roll(a, 64, 1)


def kernel(
    wsl_ref, dl_ref, el_ref, grs_ref, ces_ref, routes_ref, rate_in, hg_ref, egain_ref,
    q_hbm, k_hbm, v_hbm, gate_hbm, res_hbm, om_hbm, wg_hbm, wu_hbm, wd_hbm,
    out_ref,
    q_ref, k_ref, v_ref, gate_ref, res_ref, om_ref, wg_ref, wu_ref, wd_ref,
    small_rows, rate_ref, hgain_ref, rates, raw, kt_ref, rhs_v, rhs_k, qroll, silu_g, cols, rows_ref,
    uwbuf, mb_out, mb_in, s_out, s_in, oloc, pbuf, gated, mixed, x2,
    sel, wsel, out_buf, arrived, prod, back, xs, acc,
    load_sem, rate_sem, mb_sem, s_sem, fwd_send, fwd_recv, ret_send, ret_recv, all_in,
):
    z, x, y, c = coords()
    sp = (z << 2) + x
    partner = at(z, x, y, c + 1)

    loads = [
        pltpu.make_async_copy(src, dst, load_sem.at[i])
        for i, (src, dst) in enumerate(
            (
                (k_hbm, k_ref), (q_hbm, q_ref), (v_hbm, v_ref), (gate_hbm, gate_ref),
                (res_hbm, res_ref), (om_hbm, om_ref),
                (wg_hbm, wg_ref), (wu_hbm, wu_ref), (wd_hbm, wd_ref),
            )
        )
    ]
    for copy in loads:
        copy.start()

    barrier = pltpu.get_barrier_semaphore()

    def greet_sp(i, carry):
        pl.semaphore_signal(barrier, 1, device_id=at(z + (i >> 2), x + i, y, c), device_id_type=MESH)
        return carry

    def greet_dp(i, carry):
        pl.semaphore_signal(barrier, 1, device_id=at(z, x, y + (i >> 1), c + i), device_id_type=MESH)
        return carry

    for i in FAR:
        greet_sp(i, 0)
    for i in range(1, 8):
        greet_dp(i, 0)

    def many_recv(buf, count, sem):
        part = buf.at[pl.ds(0, count)]
        pltpu.make_async_remote_copy(part, part, sem, sem, device_id=partner, device_id_type=MESH).wait_recv()

    def many_sent(buf, count, sem):
        part = buf.at[pl.ds(0, count)]
        pltpu.make_async_remote_copy(part, part, sem, sem, device_id=partner, device_id_type=MESH).wait_send()

    lane = iota((T, T), 1)
    sub = iota((T, T), 0)
    low_half = lane < HD

    rate_ref[...] = jnp.full((8, T), rate_in[0], F32)
    hgain_ref[:, 0:HD] = hg_ref[...]
    hgain_ref[:, HD:T] = hg_ref[...]
    small_rows[...] = jnp.zeros((T, T), F32)
    small_rows[0:16, :] = wsl_ref[...]
    small_rows[16:32, :] = dl_ref[...]
    small_rows[32:48, :] = el_ref[...]
    small_rows[48:52, :] = grs_ref[...]
    small_rows[52:54, :] = ces_ref[...]
    small_rows[54:56, :] = routes_ref[...].astype(F32)
    small = jnp.transpose(small_rows[...])
    e0 = small[:, 54:55].astype(jnp.int32)
    e1 = small[:, 55:56].astype(jnp.int32)
    one0 = jnp.where(lane == e0, 1.0, 0.0)
    one1 = jnp.where(lane == e1, 1.0, 0.0)
    before = dot(jnp.where(sub > lane, 1.0, 0.0).astype(BF16), (one0 + one1).astype(BF16))
    rank0 = jnp.sum(before * one0, axis=1, keepdims=True).astype(jnp.int32)
    rank1 = jnp.sum(before * one1, axis=1, keepdims=True).astype(jnp.int32)

    def slot_of(e, rank):
        dz = ((e >> 5) - z) & 3
        dx = ((e >> 3) - x) & 3
        dy = ((e >> 1) - y) & 3
        dc = (e - c) & 1
        chunk = 3 - ((dz + dx + dy) & 3)
        return ((chunk << 5) + ((1 - dc) << 4) + ((dy ^ 2) << 2) + (dx ^ 2)) * 8 + rank

    slot0 = slot_of(e0, rank0)
    slot1 = slot_of(e1, rank1)
    scores = jnp.exp(small)
    is_group = (lane >= 48) & (lane < 52)
    is_pick = (lane >= 52) & (lane < 54)
    own_group = lane == (e0 >> 5) + 48
    group_sum = jnp.sum(jnp.where(is_group, scores, 0.0), axis=1, keepdims=True)
    group_own = jnp.sum(jnp.where(own_group, scores, 0.0), axis=1, keepdims=True)
    pick_sum = jnp.sum(jnp.where(is_pick, scores, 0.0), axis=1, keepdims=True)
    prob = group_own / group_sum
    w0 = prob * scores[:, 52:53] / pick_sum
    w1 = prob * scores[:, 53:54] / pick_sum
    wide = iota((T, NE * 8), 1)
    for h in range(2):
        w = jnp.where(wide == slot0 + 4 * h, w0, 0.0) + jnp.where(wide == slot1 + 4 * h, w1, 0.0)
        hi, lo = split(w)
        wsel[h * T : (h + 1) * T, :] = hi
        wsel[(2 + h) * T : (3 + h) * T, :] = lo
    slot_cols = jnp.where(lane == 0, slot0.astype(F32), slot1.astype(F32))
    slot_rows = jnp.transpose(slot_cols)
    row0 = slot_rows[0:1, :].astype(jnp.int32)
    row1 = slot_rows[1:2, :].astype(jnp.int32)
    tall = iota((NE * 8, T), 0)
    for h in range(2):
        hit = (tall == row0 + 4 * h) | (tall == row1 + 4 * h)
        sel[:, h * T : (h + 1) * T] = jnp.where(hit, 1.0, 0.0).astype(BF16)

    loads[0].wait()
    loads[1].wait()
    loads[2].wait()
    sums = jnp.zeros((2 * T, T), F32)
    sel_row = iota((2 * T, T), 0)
    sel_lane = iota((2 * T, T), 1)
    sel_head = (sel_row & 127) >> 6
    for j in range(NH // 2):
        cut = slice(j * T, (j + 1) * T)
        kb = k_ref[:, cut]
        qb = q_ref[:, cut]
        k32 = kb.astype(F32)
        q32 = qb.astype(F32)
        hi, lo = split(jnp.concatenate([k32 * k32, q32 * q32], axis=0))
        pick = jnp.where(sel_lane == sel_head + 2 * j, 1.0, 0.0).astype(BF16)
        sums = sums + dot(jnp.concatenate([hi, lo], axis=1), pick)
        kt = jnp.transpose(k32)
        kt_ref[j] = kt
        both = jnp.concatenate(
            [jnp.where(sub < HD, kt, 0.0), jnp.where(sub < HD, 0.0, kt)], axis=1
        ).astype(BF16)
        prods = dot(jnp.concatenate([kb, qb], axis=0), both)
        raw[2 * j] = prods[:, :T]
        raw[2 * j + 1] = prods[:, T:]
        v32 = v_ref[:, cut].astype(F32)
        kr = roll64(k32)
        rhs_v[2 * j] = jnp.where(low_half, v32, 0.0).astype(BF16)
        rhs_v[2 * j + 1] = jnp.where(low_half, 0.0, v32).astype(BF16)
        rhs_k[2 * j] = jnp.where(low_half, 0.0, kr).astype(BF16)
        rhs_k[2 * j + 1] = jnp.where(low_half, kr, 0.0).astype(BF16)
        qroll[j] = roll64(q32)
    inv = lax.rsqrt(sums + EPS)
    rk = inv[:T]
    rq = inv[T:] * (HD**-0.5)
    loads[3].wait()
    for j in range(NH // 2):
        cut = slice(j * T, (j + 1) * T)
        v32 = gate_ref[:, cut].astype(F32)
        silu_g[:, cut] = v32 / (1.0 + jnp.exp(-v32))

    pl.semaphore_wait(barrier, 22)

    def send_rate(i, carry):
        pltpu.make_async_remote_copy(
            rate_ref, rates.at[sp], rate_sem.at[0], rate_sem.at[1],
            device_id=at(z + (i >> 2), x + i, y, c), device_id_type=MESH,
        ).start()
        return carry

    for i in FAR:
        send_rate(i, 0)

    def tell_in(i, carry):
        pl.semaphore_signal(all_in, 1, device_id=at(z, x, y + (i >> 1), c + i), device_id_type=MESH)
        return carry

    for i in range(1, 8):
        tell_in(i, 0)
    rates[sp] = rate_ref[...]
    is_head = lane < NH
    beta = jax.nn.sigmoid(jnp.where(is_head, small, 0.0))
    dl = jnp.where(is_head, pltpu.roll(small, T - 16, 1), 0.0)
    el = jnp.where(is_head, pltpu.roll(small, T - 32, 1), 0.0)
    soft = jax.nn.softplus(dl)
    many_recv(rates, 15, rate_sem.at[1])
    eye16 = iota((NH, T), 0) == iota((NH, T), 1)
    rate_row = jnp.sum(jnp.where(eye16, rates[:, 0, :], 0.0), axis=0, keepdims=True)
    g = jnp.where(is_head, el - rate_row * soft, 0.0)
    g1 = g.astype(BF16)
    rest = g - g1.astype(F32)
    g2, g3 = split(rest)
    tri = jnp.where(sub >= lane, 1.0, 0.0).astype(BF16)
    cumul = dot(jnp.concatenate([tri, tri, tri], axis=1), jnp.concatenate([g1, g2, g3], axis=0))
    packed = (
        jnp.where(is_head, cumul, 0.0)
        + pltpu.roll(jnp.where(is_head, rk, 0.0), 16, 1)
        + pltpu.roll(jnp.where(is_head, beta, 0.0), 32, 1)
        + pltpu.roll(jnp.where(is_head, rq, 0.0), 48, 1)
    )
    rows_ref[...] = jnp.transpose(packed)
    colpack = (
        jnp.where(is_head, cumul, 0.0)
        + pltpu.roll(jnp.where(is_head, beta * rk, 0.0), 16, 1)
        + pltpu.roll(jnp.where(is_head, rq, 0.0), 32, 1)
    )
    cols[0] = colpack
    for n in range(1, 4):
        cols[n] = pltpu.roll(colpack, T - 4 * n, 1)

    lane64 = iota((HD, T), 1)
    sub64 = iota((HD, T), 0)

    def heads(step, carry):
        base = 8 * (((z >> 1) + 1 - step) & 1)
        causal = sub >= lane
        ls, ups, ws, kds, tots = [], [], [], [], []
        for hh in range(8):
            h = base + hh
            col = cols.at[h >> 2]
            cc = hh % 4
            c_row = rows_ref[pl.ds(h, 1), :]
            k_row = rows_ref[pl.ds(h + 16, 1), :]
            b_row = rows_ref[pl.ds(h + 32, 1), :]
            c_col = col[:, cc : cc + 1]
            dec = jnp.where(causal, jnp.exp(jnp.minimum(c_col - c_row, 0.0)), 0.0) * k_row
            ls.append(jnp.where(sub > lane, raw[h, 0:T, :] * dec * col[:, cc + 16 : cc + 17], 0.0))
            raw[h, T : 2 * T, :] = raw[h, T : 2 * T, :] * dec * col[:, cc + 32 : cc + 33]
            ups.append(b_row)
            ws.append(b_row * k_row * jnp.exp(c_row))
            last = c_row[:, T - 1 : T]
            kds.append(k_row * jnp.exp(last - c_row))
            tots.append(jnp.exp(last))
        ts = []
        pairs = (sub >> 1) == (lane >> 1)
        m = ((sub >> 1) == (lane >> 1) + 1) & (((sub >> 1) & 1) == 1)
        for l in ls:
            near = jnp.where(pairs, l, 0.0)
            far = jnp.where(m, l, 0.0)
            far = far - pltpu.roll(far, T - 1, 1) * jnp.sum(near, axis=0, keepdims=True)
            far = far - pltpu.roll(far, 1, 0) * jnp.sum(near, axis=1, keepdims=True)
            ts.append(jnp.where(sub == lane, 1.0, 0.0) - near - far)
        m = ((sub >> 2) == (lane >> 2) + 1) & (((sub >> 2) & 1) == 1)
        tsp = [split(t) for t in ts]
        xsp = [split(dot3(split(jnp.where(m, l, 0.0)), t)) for l, t in zip(ls, tsp)]
        ts = [t - dot3(tp, xx) for t, tp, xx in zip(ts, tsp, xsp)]
        for bits in range(3, 6):
            size = 1 << bits
            m = (lane64 >> bits) == 2 * (sub64 >> bits)
            none = jnp.zeros((T, T), F32)
            xs_ = [dot4(split(jnp.where(m, odd_blocks(l, size), 0.0)), split(t)) for l, t in zip(ls, ts)]
            odd = [odd_blocks(t, size) for t in ts]
            ys_ = [dot4(split(o), split(with_odd_blocks(none, x_, size))) for o, x_ in zip(odd, xs_)]
            ts = [with_odd_blocks(t, o - y_, size) for t, o, y_ in zip(ts, odd, ys_)]
        xs_ = []
        for l, t in zip(ls, ts):
            (lh, ll), (th, tl) = split(l[HD:]), split(t[:HD])
            lh32, ll32 = lh.astype(F32), ll.astype(F32)
            left = jnp.where(lane64 < HD, lh32, roll64(ll32)).astype(BF16)
            xs_.append(dot(jnp.concatenate([left, left], axis=1), jnp.concatenate([th, th, tl, tl], axis=0)))
        lowers = []
        for t, x_ in zip(ts, xs_):
            (th, tl), (xh, xl) = split(t[HD:]), split(x_)
            left = jnp.where(lane64 < HD, roll64(tl.astype(F32)), th.astype(F32)).astype(BF16)
            y_ = dot(jnp.concatenate([left, left], axis=1), jnp.concatenate([xh, xh, xl, xl], axis=0))
            lowers.append(t[HD:] - y_)
        ts = [jnp.concatenate([t[:HD], low], axis=0) for t, low in zip(ts, lowers)]
        uws = []
        for hh in range(8):
            h = base + hh
            uh, ul = split(ts[hh] * ups[hh])
            wh, wl = split(ts[hh] * ws[hh])
            vm = rhs_v[h]
            km = rhs_k[h]
            uw = dot(jnp.concatenate([uh, ul, wh, wl], axis=1), jnp.concatenate([vm, vm, km, km], axis=0))
            uws.append(split(uw))
            uwbuf[h, 0:T, :] = uws[hh][0]
            uwbuf[h, T : 2 * T, :] = uws[hh][1]
        for hh in range(8):
            h = base + hh
            ktp = kt_ref[h >> 1, (hh % 2) * HD : (hh % 2) * HD + HD, :]
            bn = dot4(split(ktp * kds[hh]), uws[hh])
            if hh % 2:
                bn = roll64(bn)
            ident = jnp.where(lane64 - HD == sub64, tots[hh], 0.0)
            mb_out[h] = jnp.where(lane64 < HD, bn, ident - bn)
        for hh in range(8):
            h = base + hh

            @pl.when(h == sp)
            def _():
                mb_in[h] = mb_out[h]

            @pl.when(h != sp)
            def _():
                pltpu.make_async_remote_copy(
                    mb_out.at[h], mb_in.at[sp], mb_sem.at[0], mb_sem.at[1],
                    device_id=at(h >> 2, hh, y, c), device_id_type=MESH,
                ).start()

        return carry

    lax.fori_loop(0, 2, heads, 0)

    def inside(n, carry):
        col = cols.at[n]
        auws = []
        for hh in range(4):
            h = n * 4 + hh
            uw = uwbuf[h]
            auws.append(dot3(split(raw[h, T : 2 * T, :]), (uw[:T], uw[T:])))
        for jj in range(2):
            j = n * 2 + jj
            a, b = 2 * jj, 2 * jj + 1
            sc_a = col[:, a + 32 : a + 33] * jnp.exp(col[:, a : a + 1])
            sc_b = col[:, b + 32 : b + 33] * jnp.exp(col[:, b : b + 1])
            p = qroll[j] * jnp.where(low_half, sc_b, sc_a) - jnp.where(low_half, auws[b], auws[a])
            hi, lo = split(p)
            pbuf[j, :, 0:T] = hi
            pbuf[j, :, T : 2 * T] = lo
            oloc[j] = jnp.where(low_half, auws[a], auws[b])
        return carry

    lax.fori_loop(0, 4, inside, 0)

    many_recv(mb_in, 15, mb_sem.at[1])
    first = lane64 < HD
    eye = (lane64 & 63) == sub64
    ident_two = jnp.where(eye, 1.0, 0.0).astype(BF16)
    ident_one = jnp.where(eye & first, 1.0, 0.0).astype(BF16)
    zero = jnp.zeros((HD, T), BF16)

    def after(later, earlier, ident):
        hi, lo = split(earlier)
        return dot4(
            later, (jnp.concatenate([ident, hi], axis=0), jnp.concatenate([zero, lo], axis=0))
        )

    def added(step):
        return jnp.where(first, step, roll64(step))

    def keep(p, state):
        s_out[p] = jnp.where(first[: HD // 2], state[: HD // 2], state[HD // 2 :]).astype(BF16)

    steps = [mb_in[p] for p in range(15)]
    ones_ = [split(m) for m in steps]
    twos = [after(ones_[2 * i + 1], steps[2 * i], ident_one) for i in range(7)]
    twos_ = [split(m) for m in twos]
    fours = [after(twos_[2 * i + 1], twos[2 * i], ident_one) for i in range(3)]
    keep(0, jnp.zeros((HD, T), F32))
    state = added(fours[0])
    keep(1, added(steps[0]))
    two = added(twos[0])
    keep(2, two)
    keep(3, after(ones_[2], two, ident_two))
    keep(4, state)
    eight = after(split(fours[1]), state, ident_two)
    six = after(twos_[2], state, ident_two)
    keep(5, after(ones_[4], state, ident_two))
    keep(6, six)
    keep(7, after(ones_[6], six, ident_two))
    keep(8, eight)
    twelve = after(split(fours[2]), eight, ident_two)
    ten = after(twos_[4], eight, ident_two)
    keep(9, after(ones_[8], eight, ident_two))
    keep(10, ten)
    fourteen = after(twos_[6], twelve, ident_two)
    keep(11, after(ones_[10], ten, ident_two))
    keep(12, twelve)
    keep(13, after(ones_[12], twelve, ident_two))
    keep(14, fourteen)
    keep(15, after(ones_[14], fourteen, ident_two))

    def send_state(i, carry):
        p = (sp + i) & 15
        pltpu.make_async_remote_copy(
            s_out.at[p], s_in.at[sp], s_sem.at[0], s_sem.at[1],
            device_id=at(p >> 2, p, y, c), device_id_type=MESH,
        ).start()
        return carry

    for i in FAR:
        send_state(i, 0)
    s_in[sp] = s_out[sp]

    many_recv(s_in, 15, s_sem.at[1])
    ones = jnp.where((iota((2 * T, T), 0) >> 6) & 1 == iota((2 * T, T), 1) >> 6, 1.0, 0.0).astype(BF16)
    for j in range(NH // 2):
        cut = slice(j * T, (j + 1) * T)
        even = s_in[2 * j].astype(F32)
        odd = s_in[2 * j + 1].astype(F32)
        head = first[: HD // 2]
        sj = jnp.concatenate(
            [
                jnp.where(head, 0.0, roll64(odd)), jnp.where(head, 0.0, odd),
                jnp.where(head, even, 0.0), jnp.where(head, roll64(even), 0.0),
            ],
            axis=0,
        ).astype(BF16)
        o = oloc[j] + dot(pbuf[j], jnp.concatenate([sj, sj], axis=0))
        hi, lo = split(o * o)
        mean = dot(jnp.concatenate([hi, lo], axis=1), ones) * (1.0 / HD)
        normed = (o * lax.rsqrt(mean + EPS) * hgain_ref[...]).astype(BF16)
        gated[:, cut] = (normed.astype(F32) * silu_g[:, cut]).astype(BF16)
    loads[4].wait()
    loads[5].wait()
    total = jnp.zeros((T, 1), F32)
    for n in range(4):
        cut = slice(n * 512, (n + 1) * 512)
        m = res_ref[:, cut].astype(F32) + dot(gated[...], om_ref[:, cut])
        mixed[:, cut] = m
        total = total + jnp.sum(m * m, axis=1, keepdims=True)
    inv = lax.rsqrt(total * (1.0 / D) + EPS)
    for h in range(2):
        cut = slice(h * HALF, (h + 1) * HALF)
        x2[h * T : (h + 1) * T, :] = (mixed[:, cut] * inv * egain_ref[:, cut]).astype(BF16)

    pl.semaphore_wait(all_in, 7)

    def dispatch(n, carry):
        block = dot(sel[pl.ds(n * 256, 256), :], x2[...]).astype(BF16)
        out_buf[pl.ds(n * PER, PER)] = block.reshape(PER, 8, HALF)

        def send(j, inner):
            i = n * PER + j
            dz, dx, dy, dc = offset(i)

            @pl.when(i != OWN)
            def _():
                pltpu.make_async_remote_copy(
                    out_buf.at[i], arrived.at[i], fwd_send, fwd_recv.at[n],
                    device_id=at(z + dz, x + dx, y + dy, c + dc), device_id_type=MESH,
                ).start()

            return inner

        lax.fori_loop(0, PER, send, 0)
        return carry

    lax.fori_loop(0, CHUNKS, dispatch, 0)
    arrived[OWN] = out_buf[OWN]
    loads[6].wait()
    loads[7].wait()
    loads[8].wait()

    sub256 = iota((256, 256), 0)
    lane256 = iota((256, 256), 1)
    source = ((sub256 & 127) >> 2) * 8 + (sub256 >> 7) * 4 + (sub256 & 3)
    apart = jnp.where(source == lane256, 1.0, 0.0).astype(BF16)
    source = ((lane256 & 127) >> 2) * 8 + (lane256 >> 7) * 4 + (lane256 & 3)
    together = jnp.where(source == sub256, 1.0, 0.0).astype(BF16)

    def send_back(n):
        def send(j, inner):
            i = n * PER + j
            dz, dx, dy, dc = offset(i)

            @pl.when(i != OWN)
            def _():
                pltpu.make_async_remote_copy(
                    prod.at[i], back.at[i], ret_send, ret_recv.at[n],
                    device_id=at(z - dz, x - dx, y - dy, c - dc), device_id_type=MESH,
                ).start()

            return inner

        lax.fori_loop(0, PER, send, 0)
    def expert(n, carry):
        @pl.when(n == 3)
        def _():
            many_recv(arrived, PER - 1, fwd_recv.at[3])

        @pl.when(n != 3)
        def _():
            many_recv(arrived, PER, fwd_recv.at[n])

        @pl.when(n >= 1)
        def _():
            send_back(n - 1)

        rows = arrived[pl.ds(n * PER, PER)].reshape(256, HALF)
        xs[...] = dot(apart, rows).astype(BF16)
        for k in range(4):
            cut = slice(k * 256, (k + 1) * 256)
            gate = dot(xs[0:T, :], wg_ref[0:HALF, cut]) + dot(xs[T : 2 * T, :], wg_ref[HALF:D, cut])
            upper = dot(xs[0:T, :], wu_ref[0:HALF, cut]) + dot(xs[T : 2 * T, :], wu_ref[HALF:D, cut])
            acc[:, cut] = (gate / (1.0 + jnp.exp(-gate)) * upper).astype(BF16)
        for k in range(8):
            cut = slice(k * 256, (k + 1) * 256)
            half, inside = k // 4, slice((k % 4) * 256, (k % 4 + 1) * 256)
            xs[half * T : (half + 1) * T, inside] = dot(acc[...], wd_ref[:, cut]).astype(BF16)
        prod[pl.ds(n * PER, PER)] = dot(together, xs[...]).astype(BF16).reshape(PER, 8, HALF)

        return carry

    lax.fori_loop(0, CHUNKS, expert, 0)
    send_back(3)
    back[OWN] = prod[OWN]

    for n in range(CHUNKS):
        many_recv(back, PER - 1 if n == 3 else PER, ret_recv.at[n])
        part = dot(wsel[:, n * 256 : (n + 1) * 256], back[n * PER : (n + 1) * PER].reshape(256, HALF))
        for h in range(2):
            cut = slice(h * HALF, (h + 1) * HALF)
            total = mixed[:, cut] + (part[h * T : (h + 1) * T] + part[(2 + h) * T : (3 + h) * T])
            if n < CHUNKS - 1:
                mixed[:, cut] = total
            else:
                out_ref[:, cut] = total.astype(BF16)

    many_sent(rates, 15, rate_sem.at[0])
    many_sent(mb_out, 15, mb_sem.at[0])
    many_sent(s_out, 15, s_sem.at[0])
    many_sent(out_buf, NE - 1, fwd_send)
    many_sent(prod, NE - 1, ret_send)


def call(*args):
    vm = pl.BlockSpec(memory_space=pltpu.VMEM)
    hbm = pl.BlockSpec(memory_space=pl.ANY)
    return pl.pallas_call(
        kernel,
        out_shape=pltpu.VMEM((T, D), BF16),
        in_specs=[vm] * 6 + [pl.BlockSpec(memory_space=pltpu.SMEM)] + [vm] * 2 + [hbm] * 9,
        out_specs=vm,
        scratch_shapes=[
            pltpu.VMEM((T, NH * HD), BF16),
            pltpu.VMEM((T, NH * HD), BF16),
            pltpu.VMEM((T, NH * HD), BF16),
            pltpu.VMEM((T, NH * HD), BF16),
            pltpu.VMEM((T, D), BF16),
            pltpu.VMEM((NH * HD, D), BF16),
            pltpu.VMEM((D, FF), BF16),
            pltpu.VMEM((D, FF), BF16),
            pltpu.VMEM((FF, D), BF16),
            pltpu.VMEM((T, T), F32),
            pltpu.VMEM((8, T), F32),
            pltpu.VMEM((1, T), F32),
            pltpu.VMEM((16, 8, T), F32),
            pltpu.VMEM((NH, 2 * T, T), F32),
            pltpu.VMEM((NH // 2, T, T), F32),
            pltpu.VMEM((NH, T, T), BF16),
            pltpu.VMEM((NH, T, T), BF16),
            pltpu.VMEM((NH // 2, T, T), F32),
            pltpu.VMEM((T, NH * HD), F32),
            pltpu.VMEM((4, T, T), F32),
            pltpu.VMEM((T, T), F32),
            pltpu.VMEM((NH, 2 * T, T), BF16),
            pltpu.VMEM((NH, HD, T), F32),
            pltpu.VMEM((NH, HD, T), F32),
            pltpu.VMEM((NH, HD // 2, T), BF16),
            pltpu.VMEM((NH, HD // 2, T), BF16),
            pltpu.VMEM((NH // 2, T, T), F32),
            pltpu.VMEM((NH // 2, T, 2 * T), BF16),
            pltpu.VMEM((T, NH * HD), BF16),
            pltpu.VMEM((T, D), F32),
            pltpu.VMEM((2 * T, HALF), BF16),
            pltpu.VMEM((NE * 8, 2 * T), BF16),
            pltpu.VMEM((4 * T, NE * 8), BF16),
            pltpu.VMEM((NE, 8, HALF), BF16),
            pltpu.VMEM((NE, 8, HALF), BF16),
            pltpu.VMEM((NE, 8, HALF), BF16),
            pltpu.VMEM((NE, 8, HALF), BF16),
            pltpu.VMEM((2 * T, HALF), BF16),
            pltpu.VMEM((T, FF), BF16),
            pltpu.SemaphoreType.DMA((9,)),
            pltpu.SemaphoreType.DMA((2,)),
            pltpu.SemaphoreType.DMA((2,)),
            pltpu.SemaphoreType.DMA((2,)),
            pltpu.SemaphoreType.DMA,
            pltpu.SemaphoreType.DMA((CHUNKS,)),
            pltpu.SemaphoreType.DMA,
            pltpu.SemaphoreType.DMA((CHUNKS,)),
            pltpu.SemaphoreType.REGULAR,
        ],
        compiler_params=pltpu.CompilerParams(
            collective_id=0, has_side_effects=True, vmem_limit_bytes=60 * 1024 * 1024
        ),
        name="layer",
    )(*args)


def shards(
    residual, query, key, value, output_gate, write_logits, decay_logits, extra_decay, head_rate,
    head_gain, output_matrix, expert_gain, group_scores, expert_scores, routes,
    gate_weight, up_weight, down_weight,
):
    out = call(
        write_logits[0].T, decay_logits[0].T, extra_decay[0].T, group_scores[0].T, expert_scores[0].T,
        routes[0].T, head_rate, head_gain[None], expert_gain[None], query[0], key[0], value[0],
        output_gate[0], residual[0], output_matrix, gate_weight[0], up_weight[0], down_weight[0],
    )
    return out[None]


def solution(mesh):
    tok = P("dp", "sp", None)
    exp = P(("sp", "dp"), None, None)
    in_specs = (
        (tok,) * 8 + (P("sp"), P(), P(), P()) + (tok,) * 3 + (exp,) * 3
    )
    return jax.shard_map(shards, mesh=mesh, in_specs=in_specs, out_specs=tok, check_vma=False)
```
